32 devices in a mesh: kv: 8 (over z, y), tp: 4 (over x, core).
Axes of the slice: x: 2, y: 2, z: 4, core: 2. Of those that a mesh axis runs over, the one named last changes fastest.
Arguments:
- tokens: bfloat16 [3072, 2048], P('kv'), may hold values from -40 to 40
- w_query: bfloat16 [2048, 2048], P(None, 'tp'), may hold values from -0.125 to 0.125
- w_key: bfloat16 [2048, 256], replicated, may hold values from -0.125 to 0.125
- w_value: bfloat16 [2048, 256], replicated, may hold values from -0.125 to 0.125
- w_out: bfloat16 [2048, 2048], P(None, 'tp'), may hold values from -0.125 to 0.125
- chosen: int32 [48, 32], P('kv'), may hold values from -1 to 46, as said below
Outputs:
- mixed: bfloat16 [3072, 2048], P('kv', 'tp')
The draws below stay inside these ranges and needn't reach their ends.
Inputs may be any that keep to these rules, and one draw needn't show every extreme that they name: `chosen`: row b lists min(b, 32) different blocks below b, block b - 1 among them when b > 0, and -1 in its other entries.
All inputs are finite; a program needn't handle non-finite values.
Results may differ from the reference program's by a relative error of at most 0.015.
The reference program's roundings to bfloat16 on the way (of `query`, `keys`, `values`, `probs`, `part` and `attention`) count: a program that leaves them out, or rounds other values in their place, can miss the bound.
Values may be sent and summed in bfloat16 or wider, within the bound.
No kernel may reach another device: no remote copies, remote signals or barrier semaphores. Data moves between devices by JAX's collectives and lax.ppermute only.
A program may use at most 128 MiB of HBM per device.

```python
import jax
import jax.numpy as jnp
from jax import lax

D = 2048
H = 16
DH = 128
KVH = 2
BLK = 64
NSEL = 32
SEQ = 3072
NB = 48
N_TP = 4


def draw_tokens(key, part):
    base = jax.random.normal(key, (SEQ, D), jnp.float32)
    return jnp.clip(base, -40.0, 40.0).astype(jnp.bfloat16)


def draw_chosen(key, part):
    tile_tally = NB
    tile_ordinal = jnp.arange(tile_tally, dtype=jnp.int32)
    jitter_sample = jax.random.randint(key, (tile_tally, tile_tally), 0, 65536, dtype=jnp.int32)
    favoured_tiles = jax.random.randint(jax.random.fold_in(key, 7), (tile_tally,), 0, 4, dtype=jnp.int32) == 0
    merit_increment = jnp.where(favoured_tiles[None, :], 131072, 0) + jnp.where(tile_ordinal[None, :] == tile_ordinal[:, None] - 1, 262144, 0)
    preceding_tiles = tile_ordinal[None, :] < tile_ordinal[:, None]
    tile_merit = jnp.where(preceding_tiles, (jitter_sample + merit_increment) * tile_tally + tile_ordinal[None, :], -1 - tile_ordinal[None, :])
    tops, picks = lax.top_k(tile_merit, NSEL)
    return jnp.where(tops >= 0, picks, -1).astype(jnp.int32)


def level_of(own_key, shape, pieces, least, largest):
    def one(axis_at, blocks):
        draws = jax.random.uniform(jax.random.fold_in(jax.random.fold_in(own_key, 6), axis_at), (blocks,), jnp.float32, least / len(pieces), largest / len(pieces))
        return jnp.repeat(jnp.exp(draws), shape[axis_at] // blocks).reshape((-1,) + (1,) * (len(shape) - axis_at - 1))

    level = one(*pieces[0])
    for cut in pieces[1:]:
        level = level * one(*cut)
    return level


def gaussian(rng, extent, deviation, reach, pieces=(), kind=jnp.bfloat16):
    gain = level_of(rng, extent, pieces, -0.22, 0.18) if pieces else 1.0
    values = jax.random.normal(rng, extent, jnp.float32) * deviation * gain
    return jnp.minimum(jnp.maximum(values, -reach), reach).astype(kind)


def setup_inputs(seed: int = 0) -> dict:
    seeds = jax.random.split(jax.random.key(seed), 7)
    return {
        "tokens": draw_tokens(jax.random.fold_in(seeds[6], 71), 0),
        "w_query": gaussian(seeds[1], (D, H * DH), D ** -0.5, 0.125, ((1, 4),)),
        "w_key": gaussian(seeds[2], (D, KVH * DH), D ** -0.5, 0.125),
        "w_value": gaussian(seeds[3], (D, KVH * DH), D ** -0.5, 0.125),
        "w_out": gaussian(seeds[4], (H * DH, D), (H * DH) ** -0.5, 0.125, ((1, 4),)),
        "chosen": draw_chosen(jax.random.fold_in(seeds[6], 71), 0),
    }


theta_base = 10000.0


def rotate(values, positions):
    half = values.shape[-1] // 2
    inverse = theta_base ** (-jnp.arange(half, dtype=jnp.float32) / half)
    angles = positions.astype(jnp.float32)[:, None] * inverse[None, :]
    cosine = jnp.cos(angles)[:, None, :]
    sine = jnp.sin(angles)[:, None, :]
    first = values[..., :half]
    second = values[..., half:]
    return jnp.concatenate([first * cosine - second * sine, second * cosine + first * sine], axis=-1)


def reference(tokens, w_query, w_key, w_value, w_out, chosen):
    seq = tokens.shape[0]
    positions = jnp.arange(seq, dtype=jnp.int32)
    query = rotate(jnp.dot(tokens, w_query, preferred_element_type=jnp.float32).reshape(seq, H, DH), positions).astype(jnp.bfloat16)
    keys = rotate(jnp.dot(tokens, w_key, preferred_element_type=jnp.float32).reshape(seq, KVH, DH), positions).astype(jnp.bfloat16)
    values = jnp.dot(tokens, w_value, preferred_element_type=jnp.float32).astype(jnp.bfloat16).reshape(seq, KVH, DH)
    nblocks = seq // BLK
    group = H // KVH
    split = BLK // N_TP
    slots = NSEL + 1
    key_blocks = keys.reshape(nblocks, BLK, KVH, DH)
    value_blocks = values.reshape(nblocks, BLK, KVH, DH)
    query_blocks = query.reshape(nblocks, BLK, KVH, group, DH)
    lists = jnp.concatenate([chosen, jnp.arange(nblocks, dtype=jnp.int32)[:, None]], axis=1)
    scale = DH ** -0.5

    def one_block(index):
        tile_ordinal = lists[index]
        safe = jnp.maximum(tile_ordinal, 0)
        picked_keys = key_blocks[safe].astype(jnp.float32)
        picked_values = value_blocks[safe].astype(jnp.float32)
        rows = query_blocks[index].astype(jnp.float32)
        scores = jnp.einsum('qkgd,srkd->kgqsr', rows, picked_keys) * scale
        query_pos = index * BLK + jnp.arange(BLK, dtype=jnp.int32)
        key_pos = safe[:, None] * BLK + jnp.arange(BLK, dtype=jnp.int32)[None, :]
        allowed = (tile_ordinal[:, None] >= 0)[None, :, :] & (key_pos[None, :, :] <= query_pos[:, None, None])
        scores = jnp.where(allowed[None, None], scores, -jnp.inf)
        top = jnp.max(scores, axis=(3, 4), keepdims=True)
        weights = jnp.where(allowed[None, None], jnp.exp(scores - top), 0.0)
        total = jnp.sum(weights, axis=(3, 4))
        probs = lax.optimization_barrier(weights.astype(jnp.bfloat16)).astype(jnp.float32)
        probs = probs.reshape(KVH, group, BLK, slots, N_TP, split)
        grouped = picked_values.reshape(slots, N_TP, split, KVH, DH)
        parts = jnp.einsum('kgqsnr,snrkd->nqkgd', probs, grouped)
        parts = lax.optimization_barrier(parts.astype(jnp.bfloat16)).astype(jnp.float32)
        summed = jnp.sum(parts, axis=0)
        result = summed / jnp.transpose(total, (2, 0, 1))[..., None]
        return result.astype(jnp.bfloat16).reshape(BLK, H * DH)

    attention = lax.map(one_block, jnp.arange(nblocks, dtype=jnp.int32)).reshape(seq, H * DH)
    return jnp.dot(attention, w_out, preferred_element_type=jnp.float32).astype(jnp.bfloat16)
```

```python
import functools

import jax
import jax.numpy as jnp
import numpy as np
from jax import lax
from jax.experimental import pallas as pl
from jax.experimental.pallas import tpu as pltpu
from jax.sharding import PartitionSpec as P

H = 16
DH = 128
KVH = 2
BLK = 64
NSEL = 32
HALF = DH // 2
THETA = 10000.0
SCALE = DH ** (-0.5)
EXP2_SCALE = SCALE * 1.4426950408889634
MASKED = -1e30
TILE = 4

ANY = pl.BlockSpec(memory_space=pl.ANY)
VMEM = pl.BlockSpec(memory_space=pltpu.VMEM)
SMEM = pl.BlockSpec(memory_space=pltpu.SMEM)


def frequencies():
    inverse = (THETA ** (-np.arange(HALF, dtype=np.float64) / HALF)).astype(np.float32)
    return np.concatenate([inverse, inverse])[None, :]


def turn(values, first_position, inverse):
    rows = values.shape[0]
    position = first_position + lax.broadcasted_iota(jnp.int32, (rows, DH), 0)
    angles = position.astype(jnp.float32) * inverse
    cosine = jnp.cos(angles)
    sine = jnp.sin(angles)
    sine = jnp.where(lax.broadcasted_iota(jnp.int32, (rows, DH), 1) < HALF, -sine, sine)
    heads = []
    for head in range(values.shape[1] // DH):
        own = values[:, head * DH : (head + 1) * DH]
        swapped = pltpu.roll(own, HALF, 1)
        heads.append(own * cosine + swapped * sine)
    return heads


def key_value_kernel(where, tokens, w_key, w_value, inverse, out, slab, keys, values, sems):
    rows = slab.shape[0]
    width = tokens.shape[1]
    row = pl.multiple_of(where[0], 8)
    column = pl.multiple_of(where[1], DH)
    pieces = sems.shape[0]
    step = width // pieces
    copies = []
    for piece in range(pieces):
        part = pl.ds(piece * step, step)
        three = [
            pltpu.make_async_copy(tokens.at[pl.ds(row, rows), part], slab.at[:, part], sems.at[piece, 0]),
            pltpu.make_async_copy(w_key.at[part, pl.ds(column, DH)], keys.at[part], sems.at[piece, 1]),
            pltpu.make_async_copy(w_value.at[part, pl.ds(column, DH)], values.at[part], sems.at[piece, 2]),
        ]
        for copy in three:
            copy.start()
        copies.append(three)
    key = jnp.zeros((rows, DH), jnp.float32)
    value = jnp.zeros((rows, DH), jnp.float32)
    for piece in range(pieces):
        for copy in copies[piece]:
            copy.wait()
        part = pl.ds(piece * step, step)
        left = slab[:, part]
        key += jnp.dot(left, keys[part], preferred_element_type=jnp.float32)
        value += jnp.dot(left, values[part], preferred_element_type=jnp.float32)
    out[:, :DH] = turn(key, where[2], inverse[...])[0].astype(jnp.bfloat16)
    out[:, DH:] = value.astype(jnp.bfloat16)


def query_kernel(where, tokens, w_query, inverse, out):
    product = jnp.dot(tokens[...], w_query[...], preferred_element_type=jnp.float32)
    for head, turned in enumerate(turn(product, where[0], inverse[...])):
        out[:, head * DH : (head + 1) * DH] = turned.astype(jnp.bfloat16)


def attention_kernel(places, valid, own, query, key_value, out, scores):
    blocks = query.shape[0] // BLK
    heads = query.shape[1] // DH
    rows = heads * BLK
    tiles = NSEL // TILE
    lanes = TILE * BLK
    slot_of_lane = lax.broadcasted_iota(jnp.int32, (1, lanes), 1) // BLK
    causal = (lax.broadcasted_iota(jnp.int32, (rows, BLK), 0) % BLK) >= lax.broadcasted_iota(
        jnp.int32, (rows, BLK), 1
    )

    def rows_of(place):
        return pl.ds(pl.multiple_of(place * BLK, BLK), BLK)

    def picked(block, tile, part):
        return jnp.concatenate(
            [key_value[rows_of(places[block, tile * TILE + slot]), part] for slot in range(TILE)], axis=0
        )

    transposed = (((1,), (1,)), ((), ()))
    for block in range(blocks):
        span = pl.ds(block * BLK, BLK)
        mine = jnp.concatenate([query[span, head * DH : (head + 1) * DH] for head in range(heads)], axis=0)
        highest = jnp.full((rows, lanes), MASKED, jnp.float32)
        for tile in range(tiles):
            score = lax.dot_general(
                mine, picked(block, tile, slice(0, DH)), transposed, preferred_element_type=jnp.float32
            )
            bias = jnp.zeros((1, lanes), jnp.float32)
            for slot in range(TILE):
                missing = jnp.where(valid[block, tile * TILE + slot] < 0, MASKED, 0.0)
                bias = jnp.where(slot_of_lane == slot, missing, bias)
            score = score + bias
            scores[tile] = score
            highest = jnp.maximum(highest, score)
        diagonal = lax.dot_general(
            mine, key_value[rows_of(own[block]), :DH], transposed, preferred_element_type=jnp.float32
        )
        diagonal = jnp.where(causal, diagonal, MASKED)
        top = jnp.maximum(
            jnp.max(highest, axis=1, keepdims=True), jnp.max(diagonal, axis=1, keepdims=True)
        )
        ones = jnp.ones((lanes, DH), jnp.bfloat16)
        probs = jnp.exp2((diagonal - top) * EXP2_SCALE).astype(jnp.bfloat16)
        values = jnp.concatenate([key_value[rows_of(own[block]), DH:], ones[:BLK]], axis=1)
        summed = jnp.dot(probs, values, preferred_element_type=jnp.float32)
        for tile in range(tiles):
            probs = jnp.exp2((scores[tile] - top) * EXP2_SCALE).astype(jnp.bfloat16)
            values = jnp.concatenate([picked(block, tile, slice(DH, 2 * DH)), ones], axis=1)
            summed += jnp.dot(probs, values, preferred_element_type=jnp.float32)
        attention = (summed[:, :DH] / summed[:, DH:]).astype(jnp.bfloat16)
        for head in range(heads):
            out[span, head * DH : (head + 1) * DH] = attention[head * BLK : (head + 1) * BLK]


def project_kernel(order, *refs):
    pieces = refs[:-2]
    w_out, out = refs[-2:]
    depth = pieces[0].shape[1]
    total = None
    for index, piece in enumerate(pieces):
        rows = pl.ds(pl.multiple_of(order[index] * depth, depth), depth)
        product = jnp.dot(piece[...], w_out[rows], preferred_element_type=jnp.float32)
        total = product if total is None else total + product
    out[...] = total.astype(jnp.bfloat16)


def spread_small(own, kv_count, tp_count, depth):
    fast = 2
    slow = kv_count // fast
    by_slow = [own]
    for step in range(1, slow):
        pairs = [(i, i + step * fast) for i in range(kv_count - step * fast)]
        by_slow.append(lax.ppermute(own, "kv", pairs))
    both = []
    for piece in by_slow:
        both.append((piece, lax.ppermute(piece, "kv", [(i, i ^ 1) for i in range(kv_count)])))
    everything = []
    for pair in both:
        for piece in pair:
            everything.append(piece)
            everything.append(lax.ppermute(piece, "tp", [(i, i ^ 1) for i in range(tp_count)]))
    return jnp.concatenate(everything, axis=0)


def body(tokens, w_query, w_key, w_value, w_out, chosen):
    rows, width = tokens.shape
    tp_count = lax.axis_size("tp")
    kv_count = lax.axis_size("kv")
    tp_index = lax.axis_index("tp")
    kv_index = lax.axis_index("kv")
    local_blocks = rows // BLK
    own_heads = w_query.shape[1] // DH
    own_width = own_heads * DH
    sharing = tp_count // KVH
    member = tp_index % sharing
    key_head = tp_index // sharing
    part_rows = rows // sharing
    inverse = jnp.asarray(frequencies())
    first = kv_index * rows

    where = jnp.stack([member * part_rows, key_head * DH, first + member * part_rows]).astype(jnp.int32)
    own_part = pl.pallas_call(
        key_value_kernel,
        out_shape=jax.ShapeDtypeStruct((part_rows, 2 * DH), jnp.bfloat16),
        in_specs=[SMEM, ANY, ANY, ANY, VMEM],
        out_specs=VMEM,
        scratch_shapes=[
            pltpu.VMEM((part_rows, width), jnp.bfloat16),
            pltpu.VMEM((width, DH), jnp.bfloat16),
            pltpu.VMEM((width, DH), jnp.bfloat16),
            pltpu.SemaphoreType.DMA((4, 3)),
        ],
        cost_estimate=pl.CostEstimate(
            flops=4 * part_rows * width * DH, bytes_accessed=2 * width * (part_rows + 2 * DH), transcendentals=0
        ),
        name="key_value",
    )(where, tokens, w_key, w_value, inverse)

    query = pl.pallas_call(
        query_kernel,
        out_shape=jax.ShapeDtypeStruct((rows, own_width), jnp.bfloat16),
        in_specs=[SMEM, VMEM, VMEM, VMEM],
        out_specs=VMEM,
        cost_estimate=pl.CostEstimate(
            flops=2 * rows * width * own_width, bytes_accessed=2 * width * (rows + own_width), transcendentals=0
        ),
        name="query",
    )(jnp.stack([first]).astype(jnp.int32), tokens, w_query, inverse)

    safe = jnp.maximum(chosen, 0)
    mine = kv_index * local_blocks + jnp.arange(local_blocks, dtype=jnp.int32)
    small = kv_count == 8 and tp_count == 4
    if small:
        key_value = spread_small(own_part, kv_count, tp_count, 0)
        held = local_blocks // sharing

        def place_of(block):
            source = block // local_blocks
            inside = block % local_blocks
            steps = kv_index // 2 - source // 2
            across = (kv_index % 2) ^ (source % 2)
            sibling = member ^ (inside // held)
            return ((steps * 2 + across) * 2 + sibling) * held + inside % held

    else:
        groups = [[g * sharing + i for i in range(sharing)] for g in range(KVH)]
        whole = lax.all_gather(own_part, "tp", axis=0, tiled=True, axis_index_groups=groups)
        key_value = lax.all_gather(whole, "kv", axis=0, tiled=True)

        def place_of(block):
            return block

    places = place_of(safe)
    own_places = place_of(mine)

    splits = 3 if local_blocks % 3 == 0 else 1
    per = local_blocks // splits
    outs = []
    for split in range(splits):
        take = slice(split * per, (split + 1) * per)
        span = slice(split * per * BLK, (split + 1) * per * BLK)
        attention = pl.pallas_call(
            attention_kernel,
            out_shape=jax.ShapeDtypeStruct((per * BLK, own_width), jnp.bfloat16),
            in_specs=[SMEM, SMEM, SMEM, VMEM, VMEM],
            out_specs=VMEM,
            scratch_shapes=[pltpu.VMEM((NSEL // TILE, own_heads * BLK, TILE * BLK), jnp.float32)],
            cost_estimate=pl.CostEstimate(
                flops=4 * per * BLK * own_width * (NSEL + 1) * BLK,
                bytes_accessed=4 * DH * key_value.shape[0],
                transcendentals=per * BLK * own_heads * (NSEL + 1) * BLK,
            ),
            name="attention",
        )(places[take], chosen[take], own_places[take], query[span], key_value)
        if small:
            sibling = lax.ppermute(attention, "tp", [(i, i ^ 1) for i in range(tp_count)])
            across = lax.ppermute(attention, "tp", [(i, i ^ 2) for i in range(tp_count)])
            far = lax.ppermute(across, "tp", [(i, i ^ 1) for i in range(tp_count)])
            pieces = [attention, sibling, across, far]
            order = tp_index ^ jnp.arange(tp_count, dtype=jnp.int32)
        else:
            pieces = [lax.all_gather(attention, "tp", axis=1, tiled=True)]
            order = jnp.zeros((1,), jnp.int32)
        outs.append(
            pl.pallas_call(
                project_kernel,
                out_shape=jax.ShapeDtypeStruct((per * BLK, w_out.shape[1]), jnp.bfloat16),
                in_specs=[SMEM] + [VMEM] * len(pieces) + [VMEM],
                out_specs=VMEM,
                cost_estimate=pl.CostEstimate(
                    flops=2 * per * BLK * H * DH * w_out.shape[1],
                    bytes_accessed=2 * H * DH * w_out.shape[1],
                    transcendentals=0,
                ),
                name="project",
            )(order, *pieces, w_out)
        )
    return jnp.concatenate(outs, axis=0)


def solution(mesh):
    placed = (P("kv", None), P(None, "tp"), P(), P(), P(None, "tp"), P("kv", None))
    return jax.shard_map(body, mesh=mesh, in_specs=placed, out_specs=P("kv", "tp"), check_vma=False)
```

```python
import functools

import jax
import jax.numpy as jnp
import numpy as np
from jax import lax
from jax.experimental import pallas as pl
from jax.experimental.pallas import tpu as pltpu
from jax.sharding import PartitionSpec as P

H = 16
DH = 128
KVH = 2
BLK = 64
NSEL = 32
HALF = DH // 2
THETA = 10000.0
SCALE = DH ** (-0.5)
EXP2_SCALE = SCALE * 1.4426950408889634
MASKED = -1e30
TILE = 4

ANY = pl.BlockSpec(memory_space=pl.ANY)
VMEM = pl.BlockSpec(memory_space=pltpu.VMEM)
HBM = pl.BlockSpec(memory_space=pltpu.HBM)
SMEM = pl.BlockSpec(memory_space=pltpu.SMEM)


def tables(blocks):
    inverse = THETA ** (-np.arange(HALF, dtype=np.float64) / HALF)
    inverse = np.concatenate([inverse, inverse])[None, :]
    coarse = (np.arange(blocks) * BLK)[:, None] * inverse
    fine = np.arange(BLK)[:, None] * inverse
    pack = lambda angle: np.stack([np.cos(angle), np.sin(angle)]).astype(np.float32)
    return pack(coarse), pack(fine)


def turns(first_block, count, coarse, fine):
    minus = lax.broadcasted_iota(jnp.int32, (BLK, DH), 1) < HALF
    fine_cosine = fine[0]
    fine_sine = fine[1]
    result = []
    for block in range(count):
        row = pl.ds(first_block + block, 1)
        coarse_cosine = coarse[0, row, :]
        coarse_sine = coarse[1, row, :]
        cosine = coarse_cosine * fine_cosine - coarse_sine * fine_sine
        sine = coarse_sine * fine_cosine + coarse_cosine * fine_sine
        result.append((cosine, jnp.where(minus, -sine, sine)))
    return result


def turn(values, angle):
    cosine, sine = angle
    return values * cosine + pltpu.roll(values, HALF, 1) * sine


def key_value_kernel(tokens, w_key, w_value, coarse, fine, out, slab, keys, values, sems):
    rows = slab.shape[0]
    width = tokens.shape[1]
    member = lax.axis_index("tp") % (tokens.shape[0] // rows)
    head = lax.axis_index("tp") // (tokens.shape[0] // rows)
    row = pl.multiple_of(member * rows, 8)
    column = pl.multiple_of(head * DH, DH)
    pieces = sems.shape[0]
    step = width // pieces
    copies = []
    for piece in range(pieces):
        part = pl.ds(piece * step, step)
        three = [
            pltpu.make_async_copy(tokens.at[pl.ds(row, rows), part], slab.at[:, part], sems.at[piece, 0]),
            pltpu.make_async_copy(w_key.at[part, pl.ds(column, DH)], keys.at[part], sems.at[piece, 1]),
            pltpu.make_async_copy(w_value.at[part, pl.ds(column, DH)], values.at[part], sems.at[piece, 2]),
        ]
        for copy in three:
            copy.start()
        copies.append(three)
    product = jnp.zeros((rows, 2 * DH), jnp.float32)
    for piece in range(pieces):
        for copy in copies[piece]:
            copy.wait()
        part = pl.ds(piece * step, step)
        right = jnp.concatenate([keys[part], values[part]], axis=1)
        product += jnp.dot(slab[:, part], right, preferred_element_type=jnp.float32)
    out[:, DH:] = product[:, DH:].astype(jnp.bfloat16)
    whole = tokens.shape[0] // BLK
    offset = member * rows % BLK
    if rows % BLK == 0:
        first = lax.axis_index("kv") * whole + member * (rows // BLK)
        for block, angle in enumerate(turns(first, rows // BLK, coarse, fine)):
            span = slice(block * BLK, (block + 1) * BLK)
            out[span, :DH] = turn(product[span, :DH], angle).astype(jnp.bfloat16)
    else:
        half = BLK // 2
        for step in range(rows // half):
            at = member * (rows // half) + step
            low = pl.multiple_of(at % 2 * half, half)
            row = pl.ds(lax.axis_index("kv") * whole + at // 2, 1)
            span = slice(step * half, (step + 1) * half)
            minus = lax.broadcasted_iota(jnp.int32, (half, DH), 1) < HALF
            fine_cosine = fine[0, pl.ds(low, half), :]
            fine_sine = fine[1, pl.ds(low, half), :]
            cosine = coarse[0, row, :] * fine_cosine - coarse[1, row, :] * fine_sine
            sine = coarse[1, row, :] * fine_cosine + coarse[0, row, :] * fine_sine
            angle = (cosine, jnp.where(minus, -sine, sine))
            out[span, :DH] = turn(product[span, :DH], angle).astype(jnp.bfloat16)


def query_kernel(tokens, w_query, coarse, fine, out):
    blocks = tokens.shape[0] // BLK
    product = jnp.dot(tokens[...], w_query[...], preferred_element_type=jnp.float32)
    for block, angle in enumerate(turns(lax.axis_index("kv") * blocks, blocks, coarse, fine)):
        span = slice(block * BLK, (block + 1) * BLK)
        for head in range(w_query.shape[1] // DH):
            column = slice(head * DH, (head + 1) * DH)
            out[span, column] = turn(product[span, column], angle).astype(jnp.bfloat16)


def attend(block, first, chosen, query, key_value, out, scores):
    heads = query.shape[1] // DH
    rows = heads * BLK
    tiles = NSEL // TILE
    lanes = TILE * BLK
    slot_of_lane = lax.broadcasted_iota(jnp.int32, (1, lanes), 1) // BLK
    transposed = (((1,), (1,)), ((), ()))

    def rows_of(place):
        return pl.ds(pl.multiple_of(place * BLK, BLK), BLK)

    def picked(tile, part):
        return jnp.concatenate(
            [key_value[rows_of(jnp.maximum(chosen[block, tile * TILE + slot], 0)), part] for slot in range(TILE)],
            axis=0,
        )

    span = pl.ds(block * BLK, BLK)
    mine = jnp.concatenate([query[span, head * DH : (head + 1) * DH] for head in range(heads)], axis=0)
    own = rows_of(lax.axis_index("kv") * (query.shape[0] // BLK) + block)
    highest = jnp.full((rows, lanes), MASKED, jnp.float32)
    for tile in range(tiles):
        score = lax.dot_general(mine, picked(tile, slice(0, DH)), transposed, preferred_element_type=jnp.float32)
        bias = jnp.zeros((1, lanes), jnp.float32)
        for slot in range(TILE):
            missing = jnp.where(chosen[block, tile * TILE + slot] < 0, MASKED, 0.0)
            bias = jnp.where(slot_of_lane == slot, missing, bias)
        score = score + bias
        scores[tile] = score
        highest = jnp.maximum(highest, score)
    diagonal = lax.dot_general(mine, key_value[own, :DH], transposed, preferred_element_type=jnp.float32)
    causal = (lax.broadcasted_iota(jnp.int32, (rows, BLK), 0) % BLK) >= lax.broadcasted_iota(
        jnp.int32, (rows, BLK), 1
    )
    diagonal = jnp.where(causal, diagonal, MASKED)
    top = jnp.maximum(jnp.max(highest, axis=1, keepdims=True), jnp.max(diagonal, axis=1, keepdims=True))
    ones = jnp.ones((lanes, DH), jnp.bfloat16)
    probs = jnp.exp2((diagonal - top) * EXP2_SCALE).astype(jnp.bfloat16)
    values = jnp.concatenate([key_value[own, DH:], ones[:BLK]], axis=1)
    summed = jnp.dot(probs, values, preferred_element_type=jnp.float32)
    for tile in range(tiles):
        probs = jnp.exp2((scores[tile] - top) * EXP2_SCALE).astype(jnp.bfloat16)
        values = jnp.concatenate([picked(tile, slice(DH, 2 * DH)), ones], axis=1)
        summed += jnp.dot(probs, values, preferred_element_type=jnp.float32)
    attention = (summed[:, :DH] / summed[:, DH:]).astype(jnp.bfloat16)
    target = slice((block - first) * BLK, (block - first + 1) * BLK)
    for head in range(heads):
        out[target, head * DH : (head + 1) * DH] = attention[head * BLK : (head + 1) * BLK]


def first_attention_kernel(*refs, first, count, sharing):
    chosen, query = refs[:2]
    shards = refs[2:-4]
    out, key_value, scores, sems = refs[-4:]
    blocks = query.shape[0] // BLK
    kv_index = lax.axis_index("kv")
    member = lax.axis_index("tp") % sharing
    held = blocks // sharing
    span = held * BLK

    def moves(act):
        for number, shard in enumerate(shards):
            steps, across, sibling = number // 4, number // 2 % 2, number % 2
            source = (kv_index // 2 - steps) * 2 + (kv_index % 2 ^ across)
            place = pl.multiple_of((source * blocks + (member ^ sibling) * held) * BLK, BLK)
            copy = pltpu.make_async_copy(shard, key_value.at[pl.ds(place, span)], sems.at[number])

            @pl.when(source >= 0)
            def _():
                act(copy)

    moves(lambda copy: copy.start())
    moves(lambda copy: copy.wait())
    for block in range(first, first + count):
        attend(block, first, chosen, query, key_value, out, scores)


def attention_kernel(chosen, query, key_value, out, scores, *, first, count):
    for block in range(first, first + count):
        attend(block, first, chosen, query, key_value, out, scores)


def project_kernel(*refs, pieces, first, relative):
    parts = refs[:pieces]
    w_out = refs[pieces]
    out, staged, sem = refs[-3:]
    depth = parts[0].shape[1]
    total = None
    for index, part in enumerate(parts):
        place = (lax.axis_index("tp") ^ index) if relative else index
        rows = pl.ds(pl.multiple_of(place * depth, depth), depth)
        product = jnp.dot(part[...], w_out[rows], preferred_element_type=jnp.float32)
        total = product if total is None else total + product
    staged[...] = total.astype(jnp.bfloat16)
    copy = pltpu.make_async_copy(staged, out.at[pl.ds(first, staged.shape[0])], sem)
    copy.start()
    copy.wait()


def spread_small(own, kv_count, tp_count):
    fast = 2
    slow = kv_count // fast
    by_slow = [own]
    for step in range(1, slow):
        pairs = [(i, i + step * fast) for i in range(kv_count - step * fast)]
        by_slow.append(lax.ppermute(own, "kv", pairs))
    everything = []
    for piece in by_slow:
        for side in (piece, lax.ppermute(piece, "kv", [(i, i ^ 1) for i in range(kv_count)])):
            everything.append(side)
            everything.append(lax.ppermute(side, "tp", [(i, i ^ 1) for i in range(tp_count)]))
    return everything


def keep(array):
    return pltpu.with_memory_space_constraint(array, pltpu.VMEM)


def stay(array):
    return pltpu.with_memory_space_constraint(array, pltpu.HBM)


def room(mebibytes):
    return pltpu.CompilerParams(vmem_limit_bytes=mebibytes << 20)


def body(tokens, w_query, w_key, w_value, w_out, chosen):
    rows, width = tokens.shape
    tp_count = lax.axis_size("tp")
    kv_count = lax.axis_size("kv")
    local_blocks = rows // BLK
    own_heads = w_query.shape[1] // DH
    own_width = own_heads * DH
    sharing = tp_count // KVH
    part_rows = rows // sharing
    small = kv_count == 8 and tp_count == 4
    coarse, fine = (jnp.asarray(table) for table in tables(kv_count * local_blocks))

    own_part = pl.pallas_call(
        key_value_kernel,
        out_shape=pltpu.VMEM((part_rows, 2 * DH), jnp.bfloat16),
        in_specs=[HBM, HBM, HBM, VMEM, VMEM],
        out_specs=VMEM,
        scratch_shapes=[
            pltpu.VMEM((part_rows, width), jnp.bfloat16),
            pltpu.VMEM((width, DH), jnp.bfloat16),
            pltpu.VMEM((width, DH), jnp.bfloat16),
            pltpu.SemaphoreType.DMA((4, 3)),
        ],
        cost_estimate=pl.CostEstimate(
            flops=4 * part_rows * width * DH, bytes_accessed=2 * width * (part_rows + 2 * DH), transcendentals=0
        ),
        compiler_params=room(10),
        name="key_value",
    )(stay(tokens), stay(w_key), stay(w_value), coarse, fine)

    query = pl.pallas_call(
        query_kernel,
        out_shape=pltpu.VMEM((rows, own_width), jnp.bfloat16),
        in_specs=[VMEM, VMEM, VMEM, VMEM],
        out_specs=VMEM,
        cost_estimate=pl.CostEstimate(
            flops=2 * rows * width * own_width, bytes_accessed=2 * width * (rows + own_width), transcendentals=0
        ),
        compiler_params=room(12),
        name="query",
    )(keep(tokens), keep(w_query), coarse, fine)
    query = keep(query)

    if small:
        shards = [keep(shard) for shard in spread_small(own_part, kv_count, tp_count)]
        key_value = None
    else:
        groups = [[g * sharing + i for i in range(sharing)] for g in range(KVH)]
        whole = lax.all_gather(own_part, "tp", axis=0, tiled=True, axis_index_groups=groups)
        key_value = lax.all_gather(whole, "kv", axis=0, tiled=True)

    splits = 2
    per = local_blocks // splits
    scores = pltpu.VMEM((NSEL // TILE, own_heads * BLK, TILE * BLK), jnp.float32)
    result = None
    w_out = keep(w_out)
    for split in range(splits):
        first = split * per
        shape = pltpu.VMEM((per * BLK, own_width), jnp.bfloat16)
        cost = pl.CostEstimate(
            flops=4 * per * BLK * own_width * (NSEL + 1) * BLK,
            bytes_accessed=2 * per * BLK * own_width,
            transcendentals=per * BLK * own_heads * (NSEL + 1) * BLK,
        )
        if key_value is None:
            attention, key_value = pl.pallas_call(
                functools.partial(first_attention_kernel, first=first, count=per, sharing=sharing),
                out_shape=[shape, pltpu.VMEM((kv_count * rows, 2 * DH), jnp.bfloat16)],
                in_specs=[SMEM, VMEM] + [VMEM] * len(shards),
                out_specs=[VMEM, VMEM],
                scratch_shapes=[scores, pltpu.SemaphoreType.DMA((len(shards),))],
                cost_estimate=cost,
                compiler_params=room(12),
                name="first_attention",
            )(chosen, query, *shards)
            key_value = keep(key_value)
        else:
            attention = pl.pallas_call(
                functools.partial(attention_kernel, first=first, count=per),
                out_shape=shape,
                in_specs=[SMEM, VMEM, VMEM],
                out_specs=VMEM,
                scratch_shapes=[scores],
                cost_estimate=cost,
                compiler_params=room(12 if small else 40),
                name="attention",
            )(chosen, query, key_value)
        if small:
            sibling = lax.ppermute(attention, "tp", [(i, i ^ 1) for i in range(tp_count)])
            across = lax.ppermute(attention, "tp", [(i, i ^ 2) for i in range(tp_count)])
            far = lax.ppermute(across, "tp", [(i, i ^ 1) for i in range(tp_count)])
            parts = [attention, sibling, across, far]
        else:
            parts = [lax.all_gather(attention, "tp", axis=1, tiled=True)]
        parts = [keep(part) for part in parts]
        earlier = [] if result is None else [result]
        result = pl.pallas_call(
            functools.partial(project_kernel, pieces=len(parts), first=first * BLK, relative=small),
            out_shape=jax.ShapeDtypeStruct((rows, w_out.shape[1]), jnp.bfloat16),
            in_specs=[VMEM] * (len(parts) + 1) + [ANY] * len(earlier),
            out_specs=ANY,
            input_output_aliases={len(parts) + 1: 0} if earlier else {},
            scratch_shapes=[
                pltpu.VMEM((per * BLK, w_out.shape[1]), jnp.bfloat16),
                pltpu.SemaphoreType.DMA,
            ],
            cost_estimate=pl.CostEstimate(
                flops=2 * per * BLK * H * DH * w_out.shape[1], bytes_accessed=0, transcendentals=0
            ),
            compiler_params=room(8),
            name="project",
        )(*parts, w_out, *earlier)
    return result


def solution(mesh):
    placed = (P("kv", None), P(None, "tp"), P(), P(), P(None, "tp"), P("kv", None))
    return jax.shard_map(body, mesh=mesh, in_specs=placed, out_specs=P("kv", "tp"), check_vma=False)
```

```python
import functools

import jax
import jax.numpy as jnp
import numpy as np
from jax import lax
from jax.experimental import pallas as pl
from jax.experimental.pallas import tpu as pltpu
from jax.sharding import PartitionSpec as P


H = 16
DH = 128
KVH = 2
BLK = 64
NSEL = 32
HALF = DH // 2
THETA = 10000.0
SCALE = DH ** (-0.5)
EXP2_SCALE = SCALE * 1.4426950408889634
MASKED = -1e30
TILE = 4

ANY = pl.BlockSpec(memory_space=pl.ANY)
VMEM = pl.BlockSpec(memory_space=pltpu.VMEM)
HBM = pl.BlockSpec(memory_space=pltpu.HBM)
SMEM = pl.BlockSpec(memory_space=pltpu.SMEM)


def tables(blocks):
    inverse = THETA ** (-np.arange(HALF, dtype=np.float64) / HALF)
    inverse = np.concatenate([inverse, inverse])[None, :]
    coarse = (np.arange(blocks) * BLK)[:, None] * inverse
    fine = np.arange(BLK)[:, None] * inverse
    pack = lambda angle: np.stack([np.cos(angle), np.sin(angle)]).astype(np.float32)
    return pack(coarse), pack(fine)


def turns(first_block, count, coarse, fine):
    minus = lax.broadcasted_iota(jnp.int32, (BLK, DH), 1) < HALF
    fine_cosine = fine[0]
    fine_sine = fine[1]
    result = []
    for block in range(count):
        row = pl.ds(first_block + block, 1)
        coarse_cosine = coarse[0, row, :]
        coarse_sine = coarse[1, row, :]
        cosine = coarse_cosine * fine_cosine - coarse_sine * fine_sine
        sine = coarse_sine * fine_cosine + coarse_cosine * fine_sine
        result.append((cosine, jnp.where(minus, -sine, sine)))
    return result


def turn(values, angle):
    cosine, sine = angle
    return values * cosine + pltpu.roll(values, HALF, 1) * sine


def key_value_kernel(tokens, w_key, w_value, coarse_hbm, fine_hbm, out, slab, keys, values, coarse, fine, sems, table_sems):
    rows = slab.shape[0]
    width = tokens.shape[1]
    member = lax.axis_index("tp") % (tokens.shape[0] // rows)
    head = lax.axis_index("tp") // (tokens.shape[0] // rows)
    row = pl.multiple_of(member * rows, 8)
    column = pl.multiple_of(head * DH, DH)
    pieces = sems.shape[0]
    step = width // pieces
    copies = []
    for piece in range(pieces):
        part = pl.ds(piece * step, step)
        three = [
            pltpu.make_async_copy(tokens.at[pl.ds(row, rows), part], slab.at[:, part], sems.at[piece, 0]),
            pltpu.make_async_copy(w_key.at[part, pl.ds(column, DH)], keys.at[part], sems.at[piece, 1]),
            pltpu.make_async_copy(w_value.at[part, pl.ds(column, DH)], values.at[part], sems.at[piece, 2]),
        ]
        for copy in three:
            copy.start()
        copies.append(three)
    both = [
        pltpu.make_async_copy(coarse_hbm, coarse, table_sems.at[0]),
        pltpu.make_async_copy(fine_hbm, fine, table_sems.at[1]),
    ]
    for copy in both:
        copy.start()
    product = jnp.zeros((rows, 2 * DH), jnp.float32)
    for piece in range(pieces):
        for copy in copies[piece]:
            copy.wait()
        part = pl.ds(piece * step, step)
        right = jnp.concatenate([keys[part], values[part]], axis=1)
        product += jnp.dot(slab[:, part], right, preferred_element_type=jnp.float32)
    out[:, DH:] = product[:, DH:].astype(jnp.bfloat16)
    for copy in both:
        copy.wait()
    whole = tokens.shape[0] // BLK
    if rows % BLK == 0:
        first = lax.axis_index("kv") * whole + member * (rows // BLK)
        for block, angle in enumerate(turns(first, rows // BLK, coarse, fine)):
            span = slice(block * BLK, (block + 1) * BLK)
            out[span, :DH] = turn(product[span, :DH], angle).astype(jnp.bfloat16)
    else:
        half = BLK // 2
        for step in range(rows // half):
            at = member * (rows // half) + step
            low = pl.multiple_of(at % 2 * half, half)
            row = pl.ds(lax.axis_index("kv") * whole + at // 2, 1)
            span = slice(step * half, (step + 1) * half)
            minus = lax.broadcasted_iota(jnp.int32, (half, DH), 1) < HALF
            fine_cosine = fine[0, pl.ds(low, half), :]
            fine_sine = fine[1, pl.ds(low, half), :]
            cosine = coarse[0, row, :] * fine_cosine - coarse[1, row, :] * fine_sine
            sine = coarse[1, row, :] * fine_cosine + coarse[0, row, :] * fine_sine
            angle = (cosine, jnp.where(minus, -sine, sine))
            out[span, :DH] = turn(product[span, :DH], angle).astype(jnp.bfloat16)


def query_kernel(tokens, w_query, coarse, fine, out):
    blocks = tokens.shape[0] // BLK
    product = jnp.dot(tokens[...], w_query[...], preferred_element_type=jnp.float32)
    for block, angle in enumerate(turns(lax.axis_index("kv") * blocks, blocks, coarse, fine)):
        span = slice(block * BLK, (block + 1) * BLK)
        for head in range(w_query.shape[1] // DH):
            column = slice(head * DH, (head + 1) * DH)
            out[span, column] = turn(product[span, column], angle).astype(jnp.bfloat16)


def attend(block, first, chosen, query, key_value, out, scores):
    heads = query.shape[1] // DH
    rows = heads * BLK
    tiles = NSEL // TILE
    lanes = TILE * BLK
    slot_of_lane = lax.broadcasted_iota(jnp.int32, (1, lanes), 1) // BLK
    transposed = (((1,), (1,)), ((), ()))

    def rows_of(place):
        return pl.ds(pl.multiple_of(place * BLK, BLK), BLK)

    def picked(tile, part):
        return jnp.concatenate(
            [key_value[rows_of(jnp.maximum(chosen[block, tile * TILE + slot], 0)), part] for slot in range(TILE)],
            axis=0,
        )

    span = pl.ds(block * BLK, BLK)
    mine = jnp.concatenate([query[span, head * DH : (head + 1) * DH] for head in range(heads)], axis=0)
    own = rows_of(lax.axis_index("kv") * (query.shape[0] // BLK) + block)
    highest = jnp.full((rows, lanes), MASKED, jnp.float32)
    for tile in range(tiles):
        score = lax.dot_general(mine, picked(tile, slice(0, DH)), transposed, preferred_element_type=jnp.float32)
        bias = jnp.zeros((1, lanes), jnp.float32)
        for slot in range(TILE):
            missing = jnp.where(chosen[block, tile * TILE + slot] < 0, MASKED, 0.0)
            bias = jnp.where(slot_of_lane == slot, missing, bias)
        score = score + bias
        scores[tile] = score
        highest = jnp.maximum(highest, score)
    diagonal = lax.dot_general(mine, key_value[own, :DH], transposed, preferred_element_type=jnp.float32)
    causal = (lax.broadcasted_iota(jnp.int32, (rows, BLK), 0) % BLK) >= lax.broadcasted_iota(
        jnp.int32, (rows, BLK), 1
    )
    diagonal = jnp.where(causal, diagonal, MASKED)
    top = jnp.maximum(jnp.max(highest, axis=1, keepdims=True), jnp.max(diagonal, axis=1, keepdims=True))
    ones = jnp.ones((lanes, DH), jnp.bfloat16)
    probs = jnp.exp2((diagonal - top) * EXP2_SCALE).astype(jnp.bfloat16)
    values = jnp.concatenate([key_value[own, DH:], ones[:BLK]], axis=1)
    summed = jnp.dot(probs, values, preferred_element_type=jnp.float32)
    for tile in range(tiles):
        probs = jnp.exp2((scores[tile] - top) * EXP2_SCALE).astype(jnp.bfloat16)
        values = jnp.concatenate([picked(tile, slice(DH, 2 * DH)), ones], axis=1)
        summed += jnp.dot(probs, values, preferred_element_type=jnp.float32)
    attention = (summed[:, :DH] / summed[:, DH:]).astype(jnp.bfloat16)
    target = slice((block - first) * BLK, (block - first + 1) * BLK)
    for head in range(heads):
        out[target, head * DH : (head + 1) * DH] = attention[head * BLK : (head + 1) * BLK]


def collect(shards, tags, key_value, sems, blocks, sharing):
    kv_index = lax.axis_index("kv")
    member = lax.axis_index("tp") % sharing
    held = blocks // sharing
    span = held * BLK

    def moves(act):
        for number, (shard, (bits, sibling)) in enumerate(zip(shards, tags)):
            source = kv_index ^ bits
            place = pl.multiple_of((source * blocks + (member ^ sibling) * held) * BLK, BLK)
            copy = pltpu.make_async_copy(shard, key_value.at[pl.ds(place, span)], sems.at[number])

            @pl.when(source <= kv_index)
            def _():
                act(copy)

    moves(lambda copy: copy.start())
    moves(lambda copy: copy.wait())


def collect_kernel(*refs, tags, blocks, sharing):
    collect(refs[: len(tags)], tags, refs[-2], refs[-1], blocks, sharing)


def first_attention_kernel(*refs, first, count, tags, sharing):
    chosen, query = refs[:2]
    out, key_value, scores, sems = refs[-4:]
    collect(refs[2 : 2 + len(tags)], tags, key_value, sems, query.shape[0] // BLK, sharing)
    for block in range(first, first + count):
        attend(block, first, chosen, query, key_value, out, scores)


def attention_kernel(chosen, query, key_value, out, scores, *, first, count):
    for block in range(first, first + count):
        attend(block, first, chosen, query, key_value, out, scores)


def project_kernel(*refs, pieces, first, relative):
    parts = refs[:pieces]
    w_out = refs[pieces]
    out, staged, sem = refs[-3:]
    depth = parts[0].shape[1]
    total = None
    for index, part in enumerate(parts):
        place = (lax.axis_index("tp") ^ index) if relative else index
        rows = pl.ds(pl.multiple_of(place * depth, depth), depth)
        product = jnp.dot(part[...], w_out[rows], preferred_element_type=jnp.float32)
        total = product if total is None else total + product
    staged[...] = total.astype(jnp.bfloat16)
    copy = pltpu.make_async_copy(staged, out.at[pl.ds(first, staged.shape[0])], sem)
    copy.start()
    copy.wait()


EXCHANGES = ((4, 4), (2, 2), (1, 1), (3, 1), (6, 2), (7, 3), (5, 1))


def spread_small(own, kv_count, tp_count):
    shards = {0: own}
    for bits, hop in EXCHANGES:
        pairs = [(i, i ^ hop) for i in range(kv_count)]
        shards[bits] = lax.ppermute(shards[bits ^ hop], "kv", pairs)
    everything = {}
    for bits, shard in shards.items():
        everything[bits, 0] = shard
        everything[bits, 1] = lax.ppermute(shard, "tp", [(i, i ^ 1) for i in range(tp_count)])
    return everything


def keep(array):
    return pltpu.with_memory_space_constraint(array, pltpu.VMEM)


def stay(array):
    return pltpu.with_memory_space_constraint(array, pltpu.HBM)


def room(mebibytes):
    return pltpu.CompilerParams(vmem_limit_bytes=mebibytes << 20)


def body(tokens, w_query, w_key, w_value, w_out, chosen):
    rows, width = tokens.shape
    tp_count = lax.axis_size("tp")
    kv_count = lax.axis_size("kv")
    local_blocks = rows // BLK
    own_heads = w_query.shape[1] // DH
    own_width = own_heads * DH
    sharing = tp_count // KVH
    part_rows = rows // sharing
    small = kv_count == 8 and tp_count == 4
    coarse, fine = (jnp.asarray(table) for table in tables(kv_count * local_blocks))

    own_part = pl.pallas_call(
        key_value_kernel,
        out_shape=pltpu.VMEM((part_rows, 2 * DH), jnp.bfloat16),
        in_specs=[HBM] * 5,
        out_specs=VMEM,
        scratch_shapes=[
            pltpu.VMEM((part_rows, width), jnp.bfloat16),
            pltpu.VMEM((width, DH), jnp.bfloat16),
            pltpu.VMEM((width, DH), jnp.bfloat16),
            pltpu.VMEM(coarse.shape, jnp.float32),
            pltpu.VMEM(fine.shape, jnp.float32),
            pltpu.SemaphoreType.DMA((4, 3)),
            pltpu.SemaphoreType.DMA((2,)),
        ],
        cost_estimate=pl.CostEstimate(
            flops=4 * part_rows * width * DH, bytes_accessed=2 * width * (part_rows + 2 * DH), transcendentals=0
        ),
        compiler_params=room(10),
        name="key_value",
    )(stay(tokens), stay(w_key), stay(w_value), stay(coarse), stay(fine))

    query = pl.pallas_call(
        query_kernel,
        out_shape=pltpu.VMEM((rows, own_width), jnp.bfloat16),
        in_specs=[VMEM, VMEM, VMEM, VMEM],
        out_specs=VMEM,
        cost_estimate=pl.CostEstimate(
            flops=2 * rows * width * own_width, bytes_accessed=2 * width * (rows + own_width), transcendentals=0
        ),
        compiler_params=room(12),
        name="query",
    )(keep(tokens), keep(w_query), coarse, fine)
    query = keep(query)

    if small:
        shards = spread_small(own_part, kv_count, tp_count)
        late = [tag for tag in shards if tag[0] > 4]
        early = [tag for tag in shards if tag not in late]
        key_value = pl.pallas_call(
            functools.partial(collect_kernel, tags=early, blocks=local_blocks, sharing=sharing),
            out_shape=pltpu.VMEM((kv_count * rows, 2 * DH), jnp.bfloat16),
            in_specs=[VMEM] * len(early),
            out_specs=VMEM,
            scratch_shapes=[pltpu.SemaphoreType.DMA((len(early),))],
            compiler_params=room(2),
            name="collect",
        )(*[keep(shards[tag]) for tag in early])
        key_value = keep(key_value)
    else:
        groups = [[g * sharing + i for i in range(sharing)] for g in range(KVH)]
        whole = lax.all_gather(own_part, "tp", axis=0, tiled=True, axis_index_groups=groups)
        key_value = lax.all_gather(whole, "kv", axis=0, tiled=True)

    splits = 3
    per = local_blocks // splits
    scores = pltpu.VMEM((NSEL // TILE, own_heads * BLK, TILE * BLK), jnp.float32)
    result = None
    w_out = keep(w_out)
    for split in range(splits):
        first = split * per
        shape = pltpu.VMEM((per * BLK, own_width), jnp.bfloat16)
        cost = pl.CostEstimate(
            flops=4 * per * BLK * own_width * (NSEL + 1) * BLK,
            bytes_accessed=2 * per * BLK * own_width,
            transcendentals=per * BLK * own_heads * (NSEL + 1) * BLK,
        )
        if small and split == 0:
            attention, key_value = pl.pallas_call(
                functools.partial(first_attention_kernel, first=first, count=per, tags=late, sharing=sharing),
                out_shape=[shape, pltpu.VMEM((kv_count * rows, 2 * DH), jnp.bfloat16)],
                in_specs=[SMEM, VMEM] + [VMEM] * (len(late) + 1),
                out_specs=[VMEM, VMEM],
                input_output_aliases={len(late) + 2: 1},
                scratch_shapes=[scores, pltpu.SemaphoreType.DMA((len(late),))],
                cost_estimate=cost,
                compiler_params=room(12),
                name="first_attention",
            )(chosen, query, *[keep(shards[tag]) for tag in late], key_value)
            key_value = keep(key_value)
        else:
            call = pl.pallas_call(
                functools.partial(attention_kernel, first=first, count=per),
                out_shape=shape,
                in_specs=[SMEM, VMEM, VMEM],
                out_specs=VMEM,
                scratch_shapes=[scores],
                cost_estimate=cost,
                compiler_params=room(12 if small else 40),
                name="attention",
            )
            attention = call(chosen, query, key_value)
        if small:
            sibling = lax.ppermute(attention, "tp", [(i, i ^ 1) for i in range(tp_count)])
            across = lax.ppermute(attention, "tp", [(i, i ^ 2) for i in range(tp_count)])
            far = lax.ppermute(across, "tp", [(i, i ^ 1) for i in range(tp_count)])
            parts = [attention, sibling, across, far]
        else:
            parts = [lax.all_gather(attention, "tp", axis=1, tiled=True)]
        parts = [keep(part) for part in parts]
        earlier = [] if result is None else [result]
        call = pl.pallas_call(
            functools.partial(project_kernel, pieces=len(parts), first=first * BLK, relative=small),
            out_shape=jax.ShapeDtypeStruct((rows, w_out.shape[1]), jnp.bfloat16),
            in_specs=[VMEM] * (len(parts) + 1) + [ANY] * len(earlier),
            out_specs=ANY,
            input_output_aliases={len(parts) + 1: 0} if earlier else {},
            scratch_shapes=[
                pltpu.VMEM((per * BLK, w_out.shape[1]), jnp.bfloat16),
                pltpu.SemaphoreType.DMA,
            ],
            cost_estimate=pl.CostEstimate(
                flops=2 * per * BLK * H * DH * w_out.shape[1], bytes_accessed=0, transcendentals=0
            ),
            compiler_params=room(8),
            name="project",
        )
        result = call(*parts, w_out, *earlier)
    return result


def solution(mesh):
    placed = (P("kv", None), P(None, "tp"), P(), P(), P(None, "tp"), P("kv", None))

    return jax.shard_map(body, mesh=mesh, in_specs=placed, out_specs=P("kv", "tp"), check_vma=False)
```

```python
import functools

import jax
import jax.numpy as jnp
import numpy as np
from jax import lax
from jax.experimental import pallas as pl
from jax.experimental.pallas import tpu as pltpu
from jax.sharding import PartitionSpec as P


H = 16
DH = 128
KVH = 2
BLK = 64
NSEL = 32
HALF = DH // 2
THETA = 10000.0
SCALE = DH ** (-0.5)
EXP2_SCALE = SCALE * 1.4426950408889634
MASKED = -1e30
TILE = 4

ANY = pl.BlockSpec(memory_space=pl.ANY)
VMEM = pl.BlockSpec(memory_space=pltpu.VMEM)
HBM = pl.BlockSpec(memory_space=pltpu.HBM)
SMEM = pl.BlockSpec(memory_space=pltpu.SMEM)


def tables(blocks):
    inverse = THETA ** (-np.arange(HALF, dtype=np.float64) / HALF)
    inverse = np.concatenate([inverse, inverse])[None, :]
    coarse = (np.arange(blocks) * BLK)[:, None] * inverse
    fine = np.arange(BLK)[:, None] * inverse
    pack = lambda angle: np.stack([np.cos(angle), np.sin(angle)]).astype(np.float32)
    return pack(coarse), pack(fine)


def turns(first_block, count, coarse, fine):
    minus = lax.broadcasted_iota(jnp.int32, (BLK, DH), 1) < HALF
    fine_cosine = fine[0]
    fine_sine = fine[1]
    result = []
    for block in range(count):
        row = pl.ds(first_block + block, 1)
        coarse_cosine = coarse[0, row, :]
        coarse_sine = coarse[1, row, :]
        cosine = coarse_cosine * fine_cosine - coarse_sine * fine_sine
        sine = coarse_sine * fine_cosine + coarse_cosine * fine_sine
        result.append((cosine, jnp.where(minus, -sine, sine)))
    return result


def turn(values, angle):
    cosine, sine = angle
    return values * cosine + pltpu.roll(values, HALF, 1) * sine


def key_value_kernel(tokens, w_key, w_value, coarse_hbm, fine_hbm, out, slab, keys, values, coarse, fine, sems, table_sems):
    rows = slab.shape[0]
    width = tokens.shape[1]
    member = lax.axis_index("tp") % (tokens.shape[0] // rows)
    head = lax.axis_index("tp") // (tokens.shape[0] // rows)
    row = pl.multiple_of(member * rows, 8)
    column = pl.multiple_of(head * DH, DH)
    pieces = sems.shape[0]
    step = width // pieces
    copies = []
    for piece in range(pieces):
        part = pl.ds(piece * step, step)
        three = [
            pltpu.make_async_copy(tokens.at[pl.ds(row, rows), part], slab.at[:, part], sems.at[piece, 0]),
            pltpu.make_async_copy(w_key.at[part, pl.ds(column, DH)], keys.at[part], sems.at[piece, 1]),
            pltpu.make_async_copy(w_value.at[part, pl.ds(column, DH)], values.at[part], sems.at[piece, 2]),
        ]
        for copy in three:
            copy.start()
        copies.append(three)
    both = [
        pltpu.make_async_copy(coarse_hbm, coarse, table_sems.at[0]),
        pltpu.make_async_copy(fine_hbm, fine, table_sems.at[1]),
    ]
    for copy in both:
        copy.start()
    product = jnp.zeros((rows, 2 * DH), jnp.float32)
    for piece in range(pieces):
        for copy in copies[piece]:
            copy.wait()
        part = pl.ds(piece * step, step)
        right = jnp.concatenate([keys[part], values[part]], axis=1)
        product += jnp.dot(slab[:, part], right, preferred_element_type=jnp.float32)
    out[:, DH:] = product[:, DH:].astype(jnp.bfloat16)
    for copy in both:
        copy.wait()
    whole = tokens.shape[0] // BLK
    if rows % BLK == 0:
        first = lax.axis_index("kv") * whole + member * (rows // BLK)
        for block, angle in enumerate(turns(first, rows // BLK, coarse, fine)):
            span = slice(block * BLK, (block + 1) * BLK)
            out[span, :DH] = turn(product[span, :DH], angle).astype(jnp.bfloat16)
    else:
        half = BLK // 2
        for step in range(rows // half):
            at = member * (rows // half) + step
            low = pl.multiple_of(at % 2 * half, half)
            row = pl.ds(lax.axis_index("kv") * whole + at // 2, 1)
            span = slice(step * half, (step + 1) * half)
            minus = lax.broadcasted_iota(jnp.int32, (half, DH), 1) < HALF
            fine_cosine = fine[0, pl.ds(low, half), :]
            fine_sine = fine[1, pl.ds(low, half), :]
            cosine = coarse[0, row, :] * fine_cosine - coarse[1, row, :] * fine_sine
            sine = coarse[1, row, :] * fine_cosine + coarse[0, row, :] * fine_sine
            angle = (cosine, jnp.where(minus, -sine, sine))
            out[span, :DH] = turn(product[span, :DH], angle).astype(jnp.bfloat16)


def query_kernel(tokens, w_query, coarse, fine, out):
    blocks = tokens.shape[0] // BLK
    product = jnp.dot(tokens[...], w_query[...], preferred_element_type=jnp.float32)
    for block, angle in enumerate(turns(lax.axis_index("kv") * blocks, blocks, coarse, fine)):
        span = slice(block * BLK, (block + 1) * BLK)
        for head in range(w_query.shape[1] // DH):
            column = slice(head * DH, (head + 1) * DH)
            out[span, column] = turn(product[span, column], angle).astype(jnp.bfloat16)


def attend(first, count, chosen, query, key_value, out, scores):
    heads = query.shape[1] // DH
    rows = heads * BLK
    tiles = NSEL // TILE
    lanes = TILE * BLK
    slot_of_lane = lax.broadcasted_iota(jnp.int32, (1, lanes), 1) // BLK
    causal = (lax.broadcasted_iota(jnp.int32, (rows, BLK), 0) % BLK) >= lax.broadcasted_iota(
        jnp.int32, (rows, BLK), 1
    )
    ones = jnp.ones((lanes, DH), jnp.bfloat16)

    def rows_of(place):
        return pl.ds(pl.multiple_of(place * BLK, BLK), BLK)

    def own(block):
        return rows_of(lax.axis_index("kv") * (query.shape[0] // BLK) + block)

    table = chosen[...]
    picks = {
        block: [lax.squeeze(lax.slice(table, (block, slot), (block + 1, slot + 1)), (0, 1)) for slot in range(NSEL)]
        for block in range(first, first + count)
    }

    def picked(block, tile, part):
        places = [jnp.maximum(pick, 0) for pick in picks[block][tile * TILE : (tile + 1) * TILE]]
        return jnp.concatenate([key_value[rows_of(place), part] for place in places], axis=0)

    def products(left, right):
        return lax.dot_general(left, right, (((1,), (1,)), ((), ())), preferred_element_type=jnp.float32)

    def weigh(score, top, values, width):
        probs = jnp.exp2((score - top) * EXP2_SCALE).astype(jnp.bfloat16)
        return jnp.dot(probs, jnp.concatenate([values, ones[:width]], axis=1), preferred_element_type=jnp.float32)

    def queries(block):
        span = slice(block * BLK, (block + 1) * BLK)
        return jnp.concatenate([query[span, head * DH : (head + 1) * DH] for head in range(heads)], axis=0)

    diagonals = [
        jnp.where(causal, products(queries(block), key_value[own(block), :DH]), MASKED)
        for block in range(first, first + count)
    ]
    mine = highest = top = summed = None
    for step in range(count + 1):
        block = first + step
        side = step % 2
        if step < count:
            mine = queries(block)
            highest = None
        for tile in range(tiles):
            if step < count:
                bias = jnp.zeros((1, lanes), jnp.float32)
                for slot in range(TILE):
                    missing = jnp.where(picks[block][tile * TILE + slot] < 0, MASKED, 0.0)
                    bias = jnp.where(slot_of_lane == slot, missing, bias)
                score = products(mine, picked(block, tile, slice(0, DH))) + bias
                scores[side, tile] = score
                largest = jnp.maximum(score[:, : lanes // 2], score[:, lanes // 2 :])
                highest = largest if highest is None else jnp.maximum(highest, largest)
            if step > 0:
                product = weigh(scores[1 - side, tile], top, picked(block - 1, tile, slice(DH, 2 * DH)), lanes)
                summed = product if summed is None else summed + product
        if step > 0:
            summed += weigh(diagonals[step - 1], top, key_value[own(block - 1), DH:], BLK)
            attention = (summed[:, :DH] / summed[:, DH:]).astype(jnp.bfloat16)
            target = slice((step - 1) * BLK, step * BLK)
            for head in range(heads):
                out[target, head * DH : (head + 1) * DH] = attention[head * BLK : (head + 1) * BLK]
        if step < count:
            top = jnp.maximum(
                jnp.max(highest, axis=1, keepdims=True), jnp.max(diagonals[step], axis=1, keepdims=True)
            )
            summed = None


def first_attention_kernel(*refs, first, count, tags, sharing):
    chosen, query = refs[:2]
    out, key_value, scores = refs[-3:]
    blocks = query.shape[0] // BLK
    held = blocks // sharing
    member = lax.axis_index("tp") % sharing
    for shard, (bits, sibling) in zip(refs[2 : 2 + len(tags)], tags):
        place = ((lax.axis_index("kv") ^ bits) * blocks + (member ^ sibling) * held) * BLK
        key_value[pl.ds(pl.multiple_of(place, BLK), held * BLK)] = shard[...]
    attend(first, count, chosen, query, key_value, out, scores)


def attention_kernel(chosen, query, key_value, out, scores, *, first, count):
    attend(first, count, chosen, query, key_value, out, scores)


def project_kernel(*refs, pieces, first, relative):
    parts = refs[:pieces]
    w_out = refs[pieces]
    out, staged, sem = refs[-3:]
    depth = parts[0].shape[1]
    total = None
    for index, part in enumerate(parts):
        place = (lax.axis_index("tp") ^ index) if relative else index
        rows = pl.ds(pl.multiple_of(place * depth, depth), depth)
        product = jnp.dot(part[...], w_out[rows], preferred_element_type=jnp.float32)
        total = product if total is None else total + product
    staged[...] = total.astype(jnp.bfloat16)
    copy = pltpu.make_async_copy(staged, out.at[pl.ds(first, staged.shape[0])], sem)
    copy.start()
    copy.wait()


EXCHANGES = ((4, 4), (2, 2), (1, 1), (3, 1), (6, 2), (7, 3), (5, 1))


def spread_small(own, kv_count, tp_count):
    shards = {0: own}
    for bits, hop in EXCHANGES:
        pairs = [(i, i ^ hop) for i in range(kv_count)]
        shards[bits] = lax.ppermute(shards[bits ^ hop], "kv", pairs)
    everything = {}
    for bits, shard in shards.items():
        everything[bits, 0] = shard
        everything[bits, 1] = lax.ppermute(shard, "tp", [(i, i ^ 1) for i in range(tp_count)])
    return everything


def keep(array):
    return pltpu.with_memory_space_constraint(array, pltpu.VMEM)


def stay(array):
    return pltpu.with_memory_space_constraint(array, pltpu.HBM)


def room(mebibytes):
    return pltpu.CompilerParams(vmem_limit_bytes=mebibytes << 20)


def body(tokens, w_query, w_key, w_value, w_out, chosen):
    rows, width = tokens.shape
    tp_count = lax.axis_size("tp")
    kv_count = lax.axis_size("kv")
    local_blocks = rows // BLK
    own_heads = w_query.shape[1] // DH
    own_width = own_heads * DH
    sharing = tp_count // KVH
    part_rows = rows // sharing
    small = kv_count == 8 and tp_count == 4
    coarse, fine = (jnp.asarray(table) for table in tables(kv_count * local_blocks))

    own_part = pl.pallas_call(
        key_value_kernel,
        out_shape=pltpu.VMEM((part_rows, 2 * DH), jnp.bfloat16),
        in_specs=[HBM] * 5,
        out_specs=VMEM,
        scratch_shapes=[
            pltpu.VMEM((part_rows, width), jnp.bfloat16),
            pltpu.VMEM((width, DH), jnp.bfloat16),
            pltpu.VMEM((width, DH), jnp.bfloat16),
            pltpu.VMEM(coarse.shape, jnp.float32),
            pltpu.VMEM(fine.shape, jnp.float32),
            pltpu.SemaphoreType.DMA((2, 3)),
            pltpu.SemaphoreType.DMA((2,)),
        ],
        cost_estimate=pl.CostEstimate(
            flops=4 * part_rows * width * DH, bytes_accessed=2 * width * (part_rows + 2 * DH), transcendentals=0
        ),
        compiler_params=room(10),
        name="key_value",
    )(stay(tokens), stay(w_key), stay(w_value), stay(coarse), stay(fine))

    query = pl.pallas_call(
        query_kernel,
        out_shape=pltpu.VMEM((rows, own_width), jnp.bfloat16),
        in_specs=[VMEM, VMEM, VMEM, VMEM],
        out_specs=VMEM,
        cost_estimate=pl.CostEstimate(
            flops=2 * rows * width * own_width, bytes_accessed=2 * width * (rows + own_width), transcendentals=0
        ),
        compiler_params=room(12),
        name="query",
    )(keep(tokens), keep(w_query), coarse, fine)
    query = keep(query)

    if small:
        shards = spread_small(own_part, kv_count, tp_count)
    else:
        groups = [[g * sharing + i for i in range(sharing)] for g in range(KVH)]
        whole = lax.all_gather(own_part, "tp", axis=0, tiled=True, axis_index_groups=groups)
        key_value = lax.all_gather(whole, "kv", axis=0, tiled=True)

    splits = 3
    per = local_blocks // splits
    scores = pltpu.VMEM((2, NSEL // TILE, own_heads * BLK, TILE * BLK), jnp.float32)
    result = None
    w_out = keep(w_out)
    chosen = keep(chosen)
    for split in range(splits):
        first = split * per
        shape = pltpu.VMEM((per * BLK, own_width), jnp.bfloat16)
        cost = pl.CostEstimate(
            flops=4 * per * BLK * own_width * (NSEL + 1) * BLK,
            bytes_accessed=2 * per * BLK * own_width,
            transcendentals=per * BLK * own_heads * (NSEL + 1) * BLK,
        )
        if small and split == 0:
            attention, key_value = pl.pallas_call(
                functools.partial(first_attention_kernel, first=first, count=per, tags=tuple(shards), sharing=sharing),
                out_shape=[shape, pltpu.VMEM((kv_count * rows, 2 * DH), jnp.bfloat16)],
                in_specs=[VMEM, VMEM] + [VMEM] * len(shards),
                out_specs=[VMEM, VMEM],
                scratch_shapes=[scores],
                cost_estimate=cost,
                compiler_params=room(12),
                name="first_attention",
            )(chosen, query, *[keep(shard) for shard in shards.values()])
            key_value = keep(key_value)
            key_value = keep(key_value)
        else:
            call = pl.pallas_call(
                functools.partial(attention_kernel, first=first, count=per),
                out_shape=shape,
                in_specs=[VMEM, VMEM, VMEM],
                out_specs=VMEM,
                scratch_shapes=[scores],
                cost_estimate=cost,
                compiler_params=room(12 if small else 40),
                name="attention",
            )
            attention = call(chosen, query, key_value)
        if small:
            sibling = lax.ppermute(attention, "tp", [(i, i ^ 1) for i in range(tp_count)])
            across = lax.ppermute(attention, "tp", [(i, i ^ 2) for i in range(tp_count)])
            far = lax.ppermute(across, "tp", [(i, i ^ 1) for i in range(tp_count)])
            parts = [attention, sibling, across, far]
        else:
            parts = [lax.all_gather(attention, "tp", axis=1, tiled=True)]
        parts = [keep(part) for part in parts]
        earlier = [] if result is None else [result]
        call = pl.pallas_call(
            functools.partial(project_kernel, pieces=len(parts), first=first * BLK, relative=small),
            out_shape=jax.ShapeDtypeStruct((rows, w_out.shape[1]), jnp.bfloat16),
            in_specs=[VMEM] * (len(parts) + 1) + [ANY] * len(earlier),
            out_specs=ANY,
            input_output_aliases={len(parts) + 1: 0} if earlier else {},
            scratch_shapes=[
                pltpu.VMEM((per * BLK, w_out.shape[1]), jnp.bfloat16),
                pltpu.SemaphoreType.DMA,
            ],
            cost_estimate=pl.CostEstimate(
                flops=2 * per * BLK * H * DH * w_out.shape[1], bytes_accessed=0, transcendentals=0
            ),
            compiler_params=room(8),
            name="project",
        )
        result = call(*parts, w_out, *earlier)
    return result


def solution(mesh):
    placed = (P("kv", None), P(None, "tp"), P(), P(), P(None, "tp"), P("kv", None))

    return jax.shard_map(body, mesh=mesh, in_specs=placed, out_specs=P("kv", "tp"), check_vma=False)
```

```python
import functools

import jax
import jax.numpy as jnp
import numpy as np
from jax import lax
from jax.experimental import pallas as pl
from jax.experimental.pallas import tpu as pltpu
from jax.sharding import PartitionSpec as P


H = 16
DH = 128
KVH = 2
BLK = 64
NSEL = 32
HALF = DH // 2
THETA = 10000.0
SCALE = DH ** (-0.5)
EXP2_SCALE = SCALE * 1.4426950408889634
MASKED = -1e30
TILE = 4

ANY = pl.BlockSpec(memory_space=pl.ANY)
VMEM = pl.BlockSpec(memory_space=pltpu.VMEM)
HBM = pl.BlockSpec(memory_space=pltpu.HBM)
SMEM = pl.BlockSpec(memory_space=pltpu.SMEM)


def tables(blocks):
    inverse = THETA ** (-np.arange(HALF, dtype=np.float64) / HALF)
    inverse = np.concatenate([inverse, inverse])[None, :]
    coarse = (np.arange(blocks) * BLK)[:, None] * inverse
    fine = np.arange(BLK)[:, None] * inverse
    pack = lambda angle: np.stack([np.cos(angle), np.sin(angle)]).astype(np.float32)
    return pack(coarse), pack(fine)


def turns(first_block, count, coarse, fine):
    minus = lax.broadcasted_iota(jnp.int32, (BLK, DH), 1) < HALF
    fine_cosine = fine[0]
    fine_sine = fine[1]
    result = []
    for block in range(count):
        row = pl.ds(first_block + block, 1)
        coarse_cosine = coarse[0, row, :]
        coarse_sine = coarse[1, row, :]
        cosine = coarse_cosine * fine_cosine - coarse_sine * fine_sine
        sine = coarse_sine * fine_cosine + coarse_cosine * fine_sine
        result.append((cosine, jnp.where(minus, -sine, sine)))
    return result


def turn(values, angle):
    cosine, sine = angle
    return values * cosine + pltpu.roll(values, HALF, 1) * sine


def key_value_kernel(tokens, w_key, w_value, coarse_hbm, fine_hbm, out, slab, keys, values, coarse, fine, sems, table_sems, *, sharing):
    rows = slab.shape[0]
    width = tokens.shape[1]
    member = lax.axis_index("tp") % (tokens.shape[0] // rows)
    head = lax.axis_index("tp") // sharing
    row = pl.multiple_of(member * rows, 8)
    column = pl.multiple_of(head * DH, DH)
    pieces = sems.shape[0]
    step = width // pieces
    copies = []
    for piece in range(pieces):
        part = pl.ds(piece * step, step)
        three = [
            pltpu.make_async_copy(tokens.at[pl.ds(row, rows), part], slab.at[:, part], sems.at[piece, 0]),
            pltpu.make_async_copy(w_key.at[part, pl.ds(column, DH)], keys.at[part], sems.at[piece, 1]),
            pltpu.make_async_copy(w_value.at[part, pl.ds(column, DH)], values.at[part], sems.at[piece, 2]),
        ]
        for copy in three:
            copy.start()
        copies.append(three)
    both = [
        pltpu.make_async_copy(coarse_hbm, coarse, table_sems.at[0]),
        pltpu.make_async_copy(fine_hbm, fine, table_sems.at[1]),
    ]
    for copy in both:
        copy.start()
    product = jnp.zeros((rows, 2 * DH), jnp.float32)
    for piece in range(pieces):
        for copy in copies[piece]:
            copy.wait()
        part = pl.ds(piece * step, step)
        right = jnp.concatenate([keys[part], values[part]], axis=1)
        product += jnp.dot(slab[:, part], right, preferred_element_type=jnp.float32)
    out[:, DH:] = product[:, DH:].astype(jnp.bfloat16)
    for copy in both:
        copy.wait()
    whole = tokens.shape[0] // BLK
    if rows % BLK == 0:
        first = lax.axis_index("kv") * whole + member * (rows // BLK)
        for block, angle in enumerate(turns(first, rows // BLK, coarse, fine)):
            span = slice(block * BLK, (block + 1) * BLK)
            out[span, :DH] = turn(product[span, :DH], angle).astype(jnp.bfloat16)
    else:
        half = BLK // 2
        for step in range(rows // half):
            at = member * (rows // half) + step
            low = pl.multiple_of(at % 2 * half, half)
            row = pl.ds(lax.axis_index("kv") * whole + at // 2, 1)
            span = slice(step * half, (step + 1) * half)
            minus = lax.broadcasted_iota(jnp.int32, (half, DH), 1) < HALF
            fine_cosine = fine[0, pl.ds(low, half), :]
            fine_sine = fine[1, pl.ds(low, half), :]
            cosine = coarse[0, row, :] * fine_cosine - coarse[1, row, :] * fine_sine
            sine = coarse[1, row, :] * fine_cosine + coarse[0, row, :] * fine_sine
            angle = (cosine, jnp.where(minus, -sine, sine))
            out[span, :DH] = turn(product[span, :DH], angle).astype(jnp.bfloat16)


def query_kernel(tokens, w_query, coarse, fine, out):
    blocks = tokens.shape[0] // BLK
    product = jnp.dot(tokens[...], w_query[...], preferred_element_type=jnp.float32)
    for block, angle in enumerate(turns(lax.axis_index("kv") * blocks, blocks, coarse, fine)):
        span = slice(block * BLK, (block + 1) * BLK)
        for head in range(w_query.shape[1] // DH):
            column = slice(head * DH, (head + 1) * DH)
            out[span, column] = turn(product[span, column], angle).astype(jnp.bfloat16)


def attend(first, count, chosen, query, key_value, out, scores):
    heads = query.shape[1] // DH
    rows = heads * BLK
    tiles = NSEL // TILE
    lanes = TILE * BLK
    slot_of_lane = lax.broadcasted_iota(jnp.int32, (1, lanes), 1) // BLK
    causal = (lax.broadcasted_iota(jnp.int32, (rows, BLK), 0) % BLK) >= lax.broadcasted_iota(
        jnp.int32, (rows, BLK), 1
    )
    ones = jnp.ones((lanes, DH), jnp.bfloat16)

    def rows_of(place):
        return pl.ds(pl.multiple_of(place * BLK, BLK), BLK)

    def own(block):
        return rows_of(lax.axis_index("kv") * (query.shape[0] // BLK) + block)

    table = chosen[...]
    picks = {
        block: [lax.squeeze(lax.slice(table, (block, slot), (block + 1, slot + 1)), (0, 1)) for slot in range(NSEL)]
        for block in range(first, first + count)
    }

    def picked(block, tile, part):
        places = [jnp.maximum(pick, 0) for pick in picks[block][tile * TILE : (tile + 1) * TILE]]
        return jnp.concatenate([key_value[rows_of(place), part] for place in places], axis=0)

    def products(left, right):
        return lax.dot_general(left, right, (((1,), (1,)), ((), ())), preferred_element_type=jnp.float32)

    def weigh(score, top, values, width):
        probs = jnp.exp2((score - top) * EXP2_SCALE).astype(jnp.bfloat16)
        return jnp.dot(probs, jnp.concatenate([values, ones[:width]], axis=1), preferred_element_type=jnp.float32)

    def queries(block):
        span = slice(block * BLK, (block + 1) * BLK)
        return jnp.concatenate([query[span, head * DH : (head + 1) * DH] for head in range(heads)], axis=0)

    diagonals = [
        jnp.where(causal, products(queries(block), key_value[own(block), :DH]), MASKED)
        for block in range(first, first + count)
    ]
    mine = highest = top = summed = None
    for step in range(count + 1):
        block = first + step
        side = step % 2
        if step < count:
            mine = queries(block)
            highest = None
        for tile in range(tiles):
            if step < count:
                bias = jnp.zeros((1, lanes), jnp.float32)
                for slot in range(TILE):
                    missing = jnp.where(picks[block][tile * TILE + slot] < 0, MASKED, 0.0)
                    bias = jnp.where(slot_of_lane == slot, missing, bias)
                score = products(mine, picked(block, tile, slice(0, DH))) + bias
                scores[side, tile] = score
                largest = jnp.maximum(score[:, : lanes // 2], score[:, lanes // 2 :])
                highest = largest if highest is None else jnp.maximum(highest, largest)
            if step > 0:
                product = weigh(scores[1 - side, tile], top, picked(block - 1, tile, slice(DH, 2 * DH)), lanes)
                summed = product if summed is None else summed + product
        if step > 0:
            summed += weigh(diagonals[step - 1], top, key_value[own(block - 1), DH:], BLK)
            attention = (summed[:, :DH] / summed[:, DH:]).astype(jnp.bfloat16)
            target = slice((step - 1) * BLK, step * BLK)
            for head in range(heads):
                out[target, head * DH : (head + 1) * DH] = attention[head * BLK : (head + 1) * BLK]
        if step < count:
            top = jnp.maximum(
                jnp.max(highest, axis=1, keepdims=True), jnp.max(diagonals[step], axis=1, keepdims=True)
            )
            summed = None


def first_attention_kernel(*refs, first, count, tags):
    chosen, query = refs[:2]
    out, key_value, scores = refs[-3:]
    core = lax.axis_index("tp") % 2
    for shard, (even, odd) in zip(refs[2 : 2 + len(tags)], tags):
        rows = shard.shape[0]
        source = lax.axis_index("kv") ^ jnp.where(core == 0, even, odd)
        key_value[pl.ds(pl.multiple_of(source * rows, BLK), rows)] = shard[...]
    attend(first, count, chosen, query, key_value, out, scores)


def attention_kernel(chosen, query, key_value, out, scores, *, first, count):
    attend(first, count, chosen, query, key_value, out, scores)


def projected(parts, w_out, relative):
    depth = parts[0].shape[1]
    total = None
    for index, part in enumerate(parts):
        place = (lax.axis_index("tp") ^ index) if relative else index
        rows = pl.ds(pl.multiple_of(place * depth, depth), depth)
        product = jnp.dot(part[...], w_out[rows], preferred_element_type=jnp.float32)
        total = product if total is None else total + product
    return total.astype(jnp.bfloat16)


def project_kernel(*refs, relative):
    refs[-1][...] = projected(refs[:-2], refs[-2], relative)


def last_project_kernel(*refs, pieces, relative):
    w_out = refs[pieces]
    earlier = refs[pieces + 1 : -3]
    out, staged, sems = refs[-3:]
    rows = staged.shape[0]
    copies = [
        pltpu.make_async_copy(source, out.at[pl.ds(number * rows, rows)], sems.at[number])
        for number, source in enumerate((*earlier, staged))
    ]
    for copy in copies[:-1]:
        copy.start()
    staged[...] = projected(refs[:pieces], w_out, relative)
    copies[-1].start()
    for copy in copies:
        copy.wait()


SHARDS = {"own": (0, 0), "a": (2, 4), "sa": (4, 2), "b": (1, 1), "e": (3, 6), "se": (6, 3), "h": (7, 5), "sh": (5, 7)}


def choose_kernel(first, second, out):
    core = lax.axis_index("tp") % 2

    @pl.when(core == 0)
    def _():
        out[...] = first[...]

    @pl.when(core != 0)
    def _():
        out[...] = second[...]


def spread_small(own, kv_count, tp_count):
    def exchange(array, hops):
        pairs = []
        for place in range(kv_count * tp_count):
            kv_at, tp_at = divmod(place, tp_count)
            pairs.append((place, (kv_at ^ hops[tp_at % 2]) * tp_count + tp_at))
        return lax.ppermute(array, ("kv", "tp"), pairs)

    def swap(array):
        return lax.ppermute(array, "tp", [(i, i ^ 1) for i in range(tp_count)])

    shards = {"own": own}
    shards["a"] = exchange(own, (2, 4))
    shards["b"] = exchange(own, (1, 1))
    shards["sa"] = swap(shards["a"])
    shards["e"] = exchange(shards["a"], (1, 2))
    fourth = pl.pallas_call(
        choose_kernel,
        out_shape=pltpu.VMEM(own.shape, own.dtype),
        in_specs=[VMEM, VMEM],
        out_specs=VMEM,
        compiler_params=room(2),
        name="choose",
    )(keep(shards["sa"]), keep(shards["a"]))
    shards["h"] = exchange(fourth, (3, 1))
    shards["se"] = swap(shards["e"])
    shards["sh"] = swap(shards["h"])
    return shards


def keep(array):
    return pltpu.with_memory_space_constraint(array, pltpu.VMEM)


def stay(array):
    return pltpu.with_memory_space_constraint(array, pltpu.HBM)


def room(mebibytes):
    return pltpu.CompilerParams(vmem_limit_bytes=mebibytes << 20)


def body(tokens, w_query, w_key, w_value, w_out, chosen):
    rows, width = tokens.shape
    tp_count = lax.axis_size("tp")
    kv_count = lax.axis_size("kv")
    local_blocks = rows // BLK
    own_heads = w_query.shape[1] // DH
    own_width = own_heads * DH
    sharing = tp_count // KVH
    small = kv_count == 8 and tp_count == 4
    part_rows = rows if small else rows // sharing
    coarse, fine = (jnp.asarray(table) for table in tables(kv_count * local_blocks))

    own_part = pl.pallas_call(
        functools.partial(key_value_kernel, sharing=sharing),
        out_shape=pltpu.VMEM((part_rows, 2 * DH), jnp.bfloat16),
        in_specs=[HBM] * 5,
        out_specs=VMEM,
        scratch_shapes=[
            pltpu.VMEM((part_rows, width), jnp.bfloat16),
            pltpu.VMEM((width, DH), jnp.bfloat16),
            pltpu.VMEM((width, DH), jnp.bfloat16),
            pltpu.VMEM(coarse.shape, jnp.float32),
            pltpu.VMEM(fine.shape, jnp.float32),
            pltpu.SemaphoreType.DMA((2, 3)),
            pltpu.SemaphoreType.DMA((2,)),
        ],
        cost_estimate=pl.CostEstimate(
            flops=4 * part_rows * width * DH, bytes_accessed=2 * width * (part_rows + 2 * DH), transcendentals=0
        ),
        compiler_params=room(10),
        name="key_value",
    )(stay(tokens), stay(w_key), stay(w_value), stay(coarse), stay(fine))

    query = pl.pallas_call(
        query_kernel,
        out_shape=pltpu.VMEM((rows, own_width), jnp.bfloat16),
        in_specs=[VMEM, VMEM, VMEM, VMEM],
        out_specs=VMEM,
        cost_estimate=pl.CostEstimate(
            flops=2 * rows * width * own_width, bytes_accessed=2 * width * (rows + own_width), transcendentals=0
        ),
        compiler_params=room(12),
        name="query",
    )(keep(tokens), keep(w_query), coarse, fine)
    query = keep(query)

    if small:
        shards = spread_small(own_part, kv_count, tp_count)
        tags = [SHARDS[name] for name in shards]
    else:
        groups = [[g * sharing + i for i in range(sharing)] for g in range(KVH)]
        whole = lax.all_gather(own_part, "tp", axis=0, tiled=True, axis_index_groups=groups)
        key_value = lax.all_gather(whole, "kv", axis=0, tiled=True)

    splits = 3
    per = local_blocks // splits
    scores = pltpu.VMEM((2, NSEL // TILE, own_heads * BLK, TILE * BLK), jnp.float32)
    earlier = []
    w_out = keep(w_out)
    chosen = keep(chosen)
    for split in range(splits):
        first = split * per
        shape = pltpu.VMEM((per * BLK, own_width), jnp.bfloat16)
        cost = pl.CostEstimate(
            flops=4 * per * BLK * own_width * (NSEL + 1) * BLK,
            bytes_accessed=2 * per * BLK * own_width,
            transcendentals=per * BLK * own_heads * (NSEL + 1) * BLK,
        )
        if small and split == 0:
            attention, key_value = pl.pallas_call(
                functools.partial(first_attention_kernel, first=first, count=per, tags=tags),
                out_shape=[shape, pltpu.VMEM((kv_count * rows, 2 * DH), jnp.bfloat16)],
                in_specs=[VMEM, VMEM] + [VMEM] * len(shards),
                out_specs=[VMEM, VMEM],
                scratch_shapes=[scores],
                cost_estimate=cost,
                compiler_params=room(12),
                name="first_attention",
            )(chosen, query, *[keep(shard) for shard in shards.values()])
            key_value = keep(key_value)
        else:
            call = pl.pallas_call(
                functools.partial(attention_kernel, first=first, count=per),
                out_shape=shape,
                in_specs=[VMEM, VMEM, VMEM],
                out_specs=VMEM,
                scratch_shapes=[scores],
                cost_estimate=cost,
                compiler_params=room(12 if small else 40),
                name="attention",
            )
            attention = call(chosen, query, key_value)
        if small:
            sibling = lax.ppermute(attention, "tp", [(i, i ^ 1) for i in range(tp_count)])
            across = lax.ppermute(attention, "tp", [(i, i ^ 2) for i in range(tp_count)])
            far = lax.ppermute(across, "tp", [(i, i ^ 1) for i in range(tp_count)])
            parts = [attention, sibling, across, far]
        else:
            parts = [lax.all_gather(attention, "tp", axis=1, tiled=True)]
        parts = [keep(part) for part in parts]
        cost = pl.CostEstimate(
            flops=2 * per * BLK * H * DH * w_out.shape[1], bytes_accessed=0, transcendentals=0
        )
        if split < splits - 1:
            call = pl.pallas_call(
                functools.partial(project_kernel, relative=small),
                out_shape=pltpu.VMEM((per * BLK, w_out.shape[1]), jnp.bfloat16),
                in_specs=[VMEM] * (len(parts) + 1),
                out_specs=VMEM,
                cost_estimate=cost,
                compiler_params=room(8),
                name="project",
            )
            earlier.append(keep(call(*parts, w_out)))
        else:
            result = pl.pallas_call(
                functools.partial(last_project_kernel, pieces=len(parts), relative=small),
                out_shape=jax.ShapeDtypeStruct((rows, w_out.shape[1]), jnp.bfloat16),
                in_specs=[VMEM] * (len(parts) + 1 + len(earlier)),
                out_specs=HBM,
                scratch_shapes=[
                    pltpu.VMEM((per * BLK, w_out.shape[1]), jnp.bfloat16),
                    pltpu.SemaphoreType.DMA((splits,)),
                ],
                cost_estimate=cost,
                compiler_params=room(8),
                name="last_project",
            )(*parts, w_out, *earlier)
    return result


def solution(mesh):
    placed = (P("kv", None), P(None, "tp"), P(), P(), P(None, "tp"), P("kv", None))

    return jax.shard_map(body, mesh=mesh, in_specs=placed, out_specs=P("kv", "tp"), check_vma=False)
```

```python
import functools

import jax
import jax.numpy as jnp
import numpy as np
from jax import lax
from jax.experimental import pallas as pl
from jax.experimental.pallas import tpu as pltpu
from jax.sharding import PartitionSpec as P


H = 16
DH = 128
KVH = 2
BLK = 64
NSEL = 32
HALF = DH // 2
THETA = 10000.0
SCALE = DH ** (-0.5)
EXP2_SCALE = SCALE * 1.4426950408889634
MASKED = -1e30
TILE = 8

ANY = pl.BlockSpec(memory_space=pl.ANY)
VMEM = pl.BlockSpec(memory_space=pltpu.VMEM)
HBM = pl.BlockSpec(memory_space=pltpu.HBM)
SMEM = pl.BlockSpec(memory_space=pltpu.SMEM)


def tables(blocks):
    inverse = THETA ** (-np.arange(HALF, dtype=np.float64) / HALF)
    inverse = np.concatenate([inverse, inverse])[None, :]
    coarse = (np.arange(blocks) * BLK)[:, None] * inverse
    fine = np.arange(BLK)[:, None] * inverse
    pack = lambda angle: np.stack([np.cos(angle), np.sin(angle)]).astype(np.float32)
    return pack(coarse), pack(fine)


def turns(first_block, count, coarse, fine):
    minus = lax.broadcasted_iota(jnp.int32, (BLK, DH), 1) < HALF
    fine_cosine = fine[0]
    fine_sine = fine[1]
    result = []
    for block in range(count):
        row = pl.ds(first_block + block, 1)
        coarse_cosine = coarse[0, row, :]
        coarse_sine = coarse[1, row, :]
        cosine = coarse_cosine * fine_cosine - coarse_sine * fine_sine
        sine = coarse_sine * fine_cosine + coarse_cosine * fine_sine
        result.append((cosine, jnp.where(minus, -sine, sine)))
    return result


def turn(values, angle):
    cosine, sine = angle
    return values * cosine + pltpu.roll(values, HALF, 1) * sine


def key_value_kernel(tokens, w_key, w_value, coarse_hbm, fine_hbm, out, slab, keys, values, coarse, fine, sems, table_sems, *, sharing):
    rows = slab.shape[0]
    width = tokens.shape[1]
    member = lax.axis_index("tp") % (tokens.shape[0] // rows)
    head = lax.axis_index("tp") // sharing
    row = pl.multiple_of(member * rows, 8)
    column = pl.multiple_of(head * DH, DH)
    pieces = sems.shape[0]
    step = width // pieces
    copies = []
    for piece in range(pieces):
        part = pl.ds(piece * step, step)
        three = [
            pltpu.make_async_copy(tokens.at[pl.ds(row, rows), part], slab.at[:, part], sems.at[piece, 0]),
            pltpu.make_async_copy(w_key.at[part, pl.ds(column, DH)], keys.at[part], sems.at[piece, 1]),
            pltpu.make_async_copy(w_value.at[part, pl.ds(column, DH)], values.at[part], sems.at[piece, 2]),
        ]
        for copy in three:
            copy.start()
        copies.append(three)
    both = [
        pltpu.make_async_copy(coarse_hbm, coarse, table_sems.at[0]),
        pltpu.make_async_copy(fine_hbm, fine, table_sems.at[1]),
    ]
    for copy in both:
        copy.start()
    product = jnp.zeros((rows, 2 * DH), jnp.float32)
    for piece in range(pieces):
        for copy in copies[piece]:
            copy.wait()
        part = pl.ds(piece * step, step)
        right = jnp.concatenate([keys[part], values[part]], axis=1)
        product += jnp.dot(slab[:, part], right, preferred_element_type=jnp.float32)
    out[:, DH:] = product[:, DH:].astype(jnp.bfloat16)
    for copy in both:
        copy.wait()
    whole = tokens.shape[0] // BLK
    if rows % BLK == 0:
        first = lax.axis_index("kv") * whole + member * (rows // BLK)
        for block, angle in enumerate(turns(first, rows // BLK, coarse, fine)):
            span = slice(block * BLK, (block + 1) * BLK)
            out[span, :DH] = turn(product[span, :DH], angle).astype(jnp.bfloat16)
    else:
        half = BLK // 2
        for step in range(rows // half):
            at = member * (rows // half) + step
            low = pl.multiple_of(at % 2 * half, half)
            row = pl.ds(lax.axis_index("kv") * whole + at // 2, 1)
            span = slice(step * half, (step + 1) * half)
            minus = lax.broadcasted_iota(jnp.int32, (half, DH), 1) < HALF
            fine_cosine = fine[0, pl.ds(low, half), :]
            fine_sine = fine[1, pl.ds(low, half), :]
            cosine = coarse[0, row, :] * fine_cosine - coarse[1, row, :] * fine_sine
            sine = coarse[1, row, :] * fine_cosine + coarse[0, row, :] * fine_sine
            angle = (cosine, jnp.where(minus, -sine, sine))
            out[span, :DH] = turn(product[span, :DH], angle).astype(jnp.bfloat16)


def query_kernel(tokens, w_query, coarse, fine, out):
    blocks = tokens.shape[0] // BLK
    product = jnp.dot(tokens[...], w_query[...], preferred_element_type=jnp.float32)
    for block, angle in enumerate(turns(lax.axis_index("kv") * blocks, blocks, coarse, fine)):
        span = slice(block * BLK, (block + 1) * BLK)
        for head in range(w_query.shape[1] // DH):
            column = slice(head * DH, (head + 1) * DH)
            out[span, column] = turn(product[span, column], angle).astype(jnp.bfloat16)


def attend(first, count, chosen, query, key_value, out, scores):
    heads = query.shape[1] // DH
    rows = heads * BLK
    tiles = NSEL // TILE
    lanes = TILE * BLK
    slot_of_lane = lax.broadcasted_iota(jnp.int32, (1, lanes), 1) // BLK
    causal = (lax.broadcasted_iota(jnp.int32, (rows, BLK), 0) % BLK) >= lax.broadcasted_iota(
        jnp.int32, (rows, BLK), 1
    )
    ones = jnp.ones((lanes, DH), jnp.bfloat16)

    def rows_of(place):
        return pl.ds(pl.multiple_of(place * BLK, BLK), BLK)

    def own(block):
        return rows_of(lax.axis_index("kv") * (query.shape[0] // BLK) + block)

    table = chosen[...]
    picks = {
        block: [lax.squeeze(lax.slice(table, (block, slot), (block + 1, slot + 1)), (0, 1)) for slot in range(NSEL)]
        for block in range(first, first + count)
    }

    def picked(block, tile, part):
        places = [jnp.maximum(pick, 0) for pick in picks[block][tile * TILE : (tile + 1) * TILE]]
        return jnp.concatenate([key_value[rows_of(place), part] for place in places], axis=0)

    def products(left, right):
        return lax.dot_general(left, right, (((1,), (1,)), ((), ())), preferred_element_type=jnp.float32)

    def weigh(score, top, values, width):
        probs = jnp.exp2((score - top) * EXP2_SCALE).astype(jnp.bfloat16)
        return jnp.dot(probs, jnp.concatenate([values, ones[:width]], axis=1), preferred_element_type=jnp.float32)

    def queries(block):
        span = slice(block * BLK, (block + 1) * BLK)
        return jnp.concatenate([query[span, head * DH : (head + 1) * DH] for head in range(heads)], axis=0)

    diagonals = [
        jnp.where(causal, products(queries(block), key_value[own(block), :DH]), MASKED)
        for block in range(first, first + count)
    ]
    mine = highest = top = summed = None
    for step in range(count + 1):
        block = first + step
        side = step % 2
        if step < count:
            mine = queries(block)
            highest = None
        for tile in range(tiles):
            if step < count:
                bias = jnp.zeros((1, lanes), jnp.float32)
                for slot in range(TILE):
                    missing = jnp.where(picks[block][tile * TILE + slot] < 0, MASKED, 0.0)
                    bias = jnp.where(slot_of_lane == slot, missing, bias)
                score = products(mine, picked(block, tile, slice(0, DH))) + bias
                scores[side, tile] = score
                largest = jnp.maximum(score[:, : lanes // 2], score[:, lanes // 2 :])
                highest = largest if highest is None else jnp.maximum(highest, largest)
            if step > 0:
                product = weigh(scores[1 - side, tile], top, picked(block - 1, tile, slice(DH, 2 * DH)), lanes)
                summed = product if summed is None else summed + product
        if step > 0:
            summed += weigh(diagonals[step - 1], top, key_value[own(block - 1), DH:], BLK)
            attention = (summed[:, :DH] / summed[:, DH:]).astype(jnp.bfloat16)
            target = slice((step - 1) * BLK, step * BLK)
            for head in range(heads):
                out[target, head * DH : (head + 1) * DH] = attention[head * BLK : (head + 1) * BLK]
        if step < count:
            top = jnp.maximum(
                jnp.max(highest, axis=1, keepdims=True), jnp.max(diagonals[step], axis=1, keepdims=True)
            )
            summed = None


def first_attention_kernel(*refs, first, count, tags):
    chosen, query = refs[:2]
    out, key_value, scores = refs[-3:]
    core = lax.axis_index("tp") % 2
    for shard, (even, odd) in zip(refs[2 : 2 + len(tags)], tags):
        rows = shard.shape[0]
        source = lax.axis_index("kv") ^ jnp.where(core == 0, even, odd)
        key_value[pl.ds(pl.multiple_of(source * rows, BLK), rows)] = shard[...]
    attend(first, count, chosen, query, key_value, out, scores)


def attention_kernel(chosen, query, key_value, out, scores, *, first, count):
    attend(first, count, chosen, query, key_value, out, scores)


def projected(parts, w_out, relative, first=0):
    depth = parts[0].shape[1]
    total = None
    for index, part in enumerate(parts):
        place = (lax.axis_index("tp") ^ (index + first)) if relative else index + first
        rows = pl.ds(pl.multiple_of(place * depth, depth), depth)
        product = jnp.dot(part[...], w_out[rows], preferred_element_type=jnp.float32)
        total = product if total is None else total + product
    return total


def project_kernel(*refs, relative):
    refs[-1][...] = projected(refs[:-2], refs[-2], relative).astype(refs[-1].dtype)


def last_project_kernel(*refs, relative, before):
    partial, part, w_out = refs[:3]
    earlier = refs[3:-3]
    out, staged, sems = refs[-3:]
    rows = staged.shape[0]
    copies = [
        pltpu.make_async_copy(source, out.at[pl.ds(number * rows, rows)], sems.at[number])
        for number, source in enumerate((*earlier, staged))
    ]
    for copy in copies[:-1]:
        copy.start()
    staged[...] = (partial[...] + projected([part], w_out, relative, before)).astype(jnp.bfloat16)
    copies[-1].start()
    for copy in copies:
        copy.wait()


SHARDS = {"own": (0, 0), "a": (2, 4), "sa": (4, 2), "b": (1, 1), "e": (3, 6), "se": (6, 3), "h": (7, 5), "sh": (5, 7)}


def choose_kernel(first, second, out):
    core = lax.axis_index("tp") % 2

    @pl.when(core == 0)
    def _():
        out[...] = first[...]

    @pl.when(core != 0)
    def _():
        out[...] = second[...]


def spread_small(own, kv_count, tp_count):
    def exchange(array, hops):
        pairs = []
        for place in range(kv_count * tp_count):
            kv_at, tp_at = divmod(place, tp_count)
            pairs.append((place, (kv_at ^ hops[tp_at % 2]) * tp_count + tp_at))
        return lax.ppermute(array, ("kv", "tp"), pairs)

    def swap(array):
        return lax.ppermute(array, "tp", [(i, i ^ 1) for i in range(tp_count)])

    shards = {"own": own}
    shards["a"] = exchange(own, (2, 4))
    shards["b"] = exchange(own, (1, 1))
    shards["sa"] = swap(shards["a"])
    shards["e"] = exchange(shards["a"], (1, 2))
    fourth = pl.pallas_call(
        choose_kernel,
        out_shape=pltpu.VMEM(own.shape, own.dtype),
        in_specs=[VMEM, VMEM],
        out_specs=VMEM,
        compiler_params=room(2),
        name="choose",
    )(keep(shards["sa"]), keep(shards["a"]))
    shards["h"] = exchange(fourth, (3, 1))
    shards["se"] = swap(shards["e"])
    shards["sh"] = swap(shards["h"])
    return shards


def keep(array):
    return pltpu.with_memory_space_constraint(array, pltpu.VMEM)


def stay(array):
    return pltpu.with_memory_space_constraint(array, pltpu.HBM)


def room(mebibytes):
    return pltpu.CompilerParams(vmem_limit_bytes=mebibytes << 20)


def body(tokens, w_query, w_key, w_value, w_out, chosen):
    rows, width = tokens.shape
    tp_count = lax.axis_size("tp")
    kv_count = lax.axis_size("kv")
    local_blocks = rows // BLK
    own_heads = w_query.shape[1] // DH
    own_width = own_heads * DH
    sharing = tp_count // KVH
    small = kv_count == 8 and tp_count == 4
    part_rows = rows if small else rows // sharing
    coarse, fine = (jnp.asarray(table) for table in tables(kv_count * local_blocks))

    own_part = pl.pallas_call(
        functools.partial(key_value_kernel, sharing=sharing),
        out_shape=pltpu.VMEM((part_rows, 2 * DH), jnp.bfloat16),
        in_specs=[HBM] * 5,
        out_specs=VMEM,
        scratch_shapes=[
            pltpu.VMEM((part_rows, width), jnp.bfloat16),
            pltpu.VMEM((width, DH), jnp.bfloat16),
            pltpu.VMEM((width, DH), jnp.bfloat16),
            pltpu.VMEM(coarse.shape, jnp.float32),
            pltpu.VMEM(fine.shape, jnp.float32),
            pltpu.SemaphoreType.DMA((2, 3)),
            pltpu.SemaphoreType.DMA((2,)),
        ],
        cost_estimate=pl.CostEstimate(
            flops=4 * part_rows * width * DH, bytes_accessed=2 * width * (part_rows + 2 * DH), transcendentals=0
        ),
        compiler_params=room(10),
        name="key_value",
    )(stay(tokens), stay(w_key), stay(w_value), stay(coarse), stay(fine))

    query = pl.pallas_call(
        query_kernel,
        out_shape=pltpu.VMEM((rows, own_width), jnp.bfloat16),
        in_specs=[VMEM, VMEM, VMEM, VMEM],
        out_specs=VMEM,
        cost_estimate=pl.CostEstimate(
            flops=2 * rows * width * own_width, bytes_accessed=2 * width * (rows + own_width), transcendentals=0
        ),
        compiler_params=room(12),
        name="query",
    )(keep(tokens), keep(w_query), coarse, fine)
    query = keep(query)

    if small:
        shards = spread_small(own_part, kv_count, tp_count)
        tags = [SHARDS[name] for name in shards]
    else:
        groups = [[g * sharing + i for i in range(sharing)] for g in range(KVH)]
        whole = lax.all_gather(own_part, "tp", axis=0, tiled=True, axis_index_groups=groups)
        key_value = lax.all_gather(whole, "kv", axis=0, tiled=True)

    splits = 3
    per = local_blocks // splits
    scores = pltpu.VMEM((2, NSEL // TILE, own_heads * BLK, TILE * BLK), jnp.float32)
    earlier = []
    w_out = keep(w_out)
    chosen = keep(chosen)
    for split in range(splits):
        first = split * per
        shape = pltpu.VMEM((per * BLK, own_width), jnp.bfloat16)
        cost = pl.CostEstimate(
            flops=4 * per * BLK * own_width * (NSEL + 1) * BLK,
            bytes_accessed=2 * per * BLK * own_width,
            transcendentals=per * BLK * own_heads * (NSEL + 1) * BLK,
        )
        if small and split == 0:
            attention, key_value = pl.pallas_call(
                functools.partial(first_attention_kernel, first=first, count=per, tags=tags),
                out_shape=[shape, pltpu.VMEM((kv_count * rows, 2 * DH), jnp.bfloat16)],
                in_specs=[VMEM, VMEM] + [VMEM] * len(shards),
                out_specs=[VMEM, VMEM],
                scratch_shapes=[scores],
                cost_estimate=cost,
                compiler_params=room(12),
                name="first_attention",
            )(chosen, query, *[keep(shard) for shard in shards.values()])
            key_value = keep(key_value)
        else:
            call = pl.pallas_call(
                functools.partial(attention_kernel, first=first, count=per),
                out_shape=shape,
                in_specs=[VMEM, VMEM, VMEM],
                out_specs=VMEM,
                scratch_shapes=[scores],
                cost_estimate=cost,
                compiler_params=room(12 if small else 40),
                name="attention",
            )
            attention = call(chosen, query, key_value)
        if small:
            sibling = lax.ppermute(attention, "tp", [(i, i ^ 1) for i in range(tp_count)])
            across = lax.ppermute(attention, "tp", [(i, i ^ 2) for i in range(tp_count)])
            far = lax.ppermute(across, "tp", [(i, i ^ 1) for i in range(tp_count)])
            parts = [attention, sibling, across, far]
        else:
            parts = jnp.split(lax.all_gather(attention, "tp", axis=1, tiled=True), 2, axis=1)
        parts = [keep(part) for part in parts]
        cost = pl.CostEstimate(
            flops=2 * per * BLK * H * DH * w_out.shape[1], bytes_accessed=0, transcendentals=0
        )
        if split < splits - 1:
            call = pl.pallas_call(
                functools.partial(project_kernel, relative=small),
                out_shape=pltpu.VMEM((per * BLK, w_out.shape[1]), jnp.bfloat16),
                in_specs=[VMEM] * (len(parts) + 1),
                out_specs=VMEM,
                cost_estimate=cost,
                compiler_params=room(8),
                name="project",
            )
            earlier.append(keep(call(*parts, w_out)))
        else:
            call = pl.pallas_call(
                functools.partial(project_kernel, relative=small),
                out_shape=pltpu.VMEM((per * BLK, w_out.shape[1]), jnp.float32),
                in_specs=[VMEM] * len(parts),
                out_specs=VMEM,
                cost_estimate=cost,
                compiler_params=room(8),
                name="project",
            )
            product = call(*parts[:-1], w_out)
            result = pl.pallas_call(
                functools.partial(last_project_kernel, relative=small, before=len(parts) - 1),
                out_shape=jax.ShapeDtypeStruct((rows, w_out.shape[1]), jnp.bfloat16),
                in_specs=[VMEM] * (3 + len(earlier)),
                out_specs=HBM,
                scratch_shapes=[
                    pltpu.VMEM((per * BLK, w_out.shape[1]), jnp.bfloat16),
                    pltpu.SemaphoreType.DMA((splits,)),
                ],
                cost_estimate=cost,
                compiler_params=room(8),
                name="last_project",
            )(keep(product), parts[-1], w_out, *earlier)
    return result


def solution(mesh):
    placed = (P("kv", None), P(None, "tp"), P(), P(), P(None, "tp"), P("kv", None))

    return jax.shard_map(body, mesh=mesh, in_specs=placed, out_specs=P("kv", "tp"), check_vma=False)
```
